32 devices in a mesh: fs: 4 (over z), tp: 4 (over y, x), rep: 2 (over core).
Axes of the slice: x: 2, y: 2, z: 4, core: 2. Of those that a mesh axis runs over, the one named last changes fastest.
Arguments:
- gate_grads: float32 [2, 5632, 2048], P('rep', 'fs', 'tp'), may hold values from -16 to 16, as said below
- gate_velocity: float32 [5632, 2048], P(('fs', 'rep'), 'tp'), may hold values from -31 to 31, as said below
- gate_weight: float32 [5632, 2048], P(('fs', 'rep'), 'tp'), may hold values from -4 to 4
- up_grads: float32 [2, 5632, 2048], P('rep', 'fs', 'tp'), may hold values from -16 to 16, as said below
- up_velocity: float32 [5632, 2048], P(('fs', 'rep'), 'tp'), may hold values from -31 to 31, as said below
- up_weight: float32 [5632, 2048], P(('fs', 'rep'), 'tp'), may hold values from -4 to 4
- branch_grads: float32 [2, 2048, 1024], P('rep', 'fs', 'tp'), may hold values from -16 to 16, as said below
- branch_velocity: float32 [2048, 1024], P(('fs', 'rep'), 'tp'), may hold values from -31 to 31, as said below
- branch_weight: float32 [2048, 1024], P(('fs', 'rep'), 'tp'), may hold values from -4 to 4
Outputs:
- gate_momentum: float32 [5632, 2048], P(('fs', 'rep'), 'tp')
- gate_updated: float32 [5632, 2048], P(('fs', 'rep'), 'tp')
- up_momentum: float32 [5632, 2048], P(('fs', 'rep'), 'tp')
- up_updated: float32 [5632, 2048], P(('fs', 'rep'), 'tp')
- branch_momentum: float32 [2048, 1024], P(('fs', 'rep'), 'tp')
- branch_updated: float32 [2048, 1024], P(('fs', 'rep'), 'tp')
The draws below stay inside these ranges and needn't reach their ends.
Inputs may be any that keep to these rules, and one draw needn't show every extreme that they name: `gate_grads`: entries vary in scale over rows and over columns. `up_grads`: entries vary in scale over rows and over columns. `branch_grads`: entries vary in scale over rows and over columns. `gate_velocity`: entries vary in scale over rows and over columns. `up_velocity`: entries vary in scale over rows and over columns. `branch_velocity`: entries vary in scale over rows and over columns.
All inputs are finite; a program needn't handle non-finite values.
Results may differ from the reference program's by a relative error of at most 0.039.
Values may be sent and summed in bfloat16 or wider, within the bound.
A program may use at most 64 MiB of HBM per device.

```python
import math
import jax
import jax.numpy as jnp
from jax import lax

D = 2048
FF = 5632
BRANCH = 1024
ITERS = 3
REP = 2
N_FS = 4
N_REP = 2


def block_scaled(key, height, width):
    noise_key, row_key, col_key = jax.random.split(key, 3)
    noise = jnp.clip(jax.random.normal(noise_key, (height, width), jnp.float32), -4.0, 4.0)
    rise = math.log(4.0)
    row_factor = jnp.exp(jax.random.uniform(row_key, (8,), jnp.float32, -0.3, 0.3))
    col_factor = jnp.exp(jax.random.uniform(col_key, (4,), jnp.float32, -0.3, 0.3))
    row_ramp = jnp.exp(rise * (jnp.arange(height, dtype=jnp.float32) / (height - 1) - 1.0))
    col_ramp = jnp.exp(rise * (jnp.arange(width, dtype=jnp.float32) / (width - 1) - 1.0))
    row_scale = jnp.repeat(row_factor, height // 8) * row_ramp
    col_scale = jnp.repeat(col_factor, width // 4) * col_ramp
    return noise * row_scale[:, None] * col_scale[None, :]


def replicas(key, height, width):
    return jnp.stack([block_scaled(jax.random.fold_in(key, 11 + index), height, width) for index in range(REP)])


def draw_gate_grads(key, part):
    return replicas(key, FF, D)


def draw_up_grads(key, part):
    return replicas(jax.random.fold_in(key, 3), FF, D)


def draw_branch_grads(key, part):
    return replicas(jax.random.fold_in(key, 5), D, BRANCH)


def draw_gate_velocity(key, part):
    return 2.0 * block_scaled(jax.random.fold_in(key, 21), FF, D)


def draw_up_velocity(key, part):
    return 2.0 * block_scaled(jax.random.fold_in(key, 23), FF, D)


def draw_branch_velocity(key, part):
    return 2.0 * block_scaled(jax.random.fold_in(key, 25), D, BRANCH)


def steps_of(key, extent, cuts, smallest, high):
    def one(dim, parts):
        steps = jax.random.uniform(jax.random.fold_in(jax.random.fold_in(key, 6), dim), (parts,), jnp.float32, smallest / len(cuts), high / len(cuts))
        return jnp.repeat(jnp.exp(steps), extent[dim] // parts).reshape((-1,) + (1,) * (len(extent) - dim - 1))

    gain = one(*cuts[0])
    for cut in cuts[1:]:
        gain = gain * one(*cut)
    return gain


def normal_values(own_key, shape, scale, most, shards=(), kind=jnp.bfloat16):
    array = jax.random.normal(own_key, shape, jnp.float32) * scale
    if len(shards) > 0:
        array = steps_of(own_key, shape, shards, -0.22, 0.18) * array
    return jnp.clip(array, min=-most, max=most).astype(kind)


def setup_inputs(seed: int = 0) -> dict:
    keys = jax.random.split(jax.random.key(seed), 10)
    return {
        "gate_grads": draw_gate_grads(jax.random.fold_in(keys[9], 71), 0),
        "gate_velocity": draw_gate_velocity(jax.random.fold_in(keys[9], 71), 0),
        "gate_weight": normal_values(keys[2], (FF, D), 1.0, 4.0, ((0, 8), (1, 4)), jnp.float32),
        "up_grads": draw_up_grads(jax.random.fold_in(keys[9], 71), 0),
        "up_velocity": draw_up_velocity(jax.random.fold_in(keys[9], 71), 0),
        "up_weight": normal_values(keys[5], (FF, D), 1.0, 4.0, ((0, 8), (1, 4)), jnp.float32),
        "branch_grads": draw_branch_grads(jax.random.fold_in(keys[9], 71), 0),
        "branch_velocity": draw_branch_velocity(jax.random.fold_in(keys[9], 71), 0),
        "branch_weight": normal_values(keys[8], (D, BRANCH), 1.0, 4.0, ((0, 8), (1, 4)), jnp.float32),
    }


MOMENT = 0.95
COEF_ONE = 3.4445
COEF_THREE = -4.775
COEF_FIVE = 2.0315
SAFETY = 2.0
RATE = 0.5
SHRINK = 0.95

def block_gram(matrix):
    count = N_FS * N_REP
    height = matrix.shape[0] // count
    width = matrix.shape[1]
    stacked = matrix.reshape(count, height, width)

    def add_block(total, block):
        part = jnp.dot(block.T, block, preferred_element_type=jnp.float32)
        narrow = lax.optimization_barrier(part.astype(jnp.bfloat16))
        return (total + narrow.astype(jnp.float32), None)
    total, unused = lax.scan(add_block, jnp.zeros((width, width), jnp.float32), stacked)
    return total

def orthogonal(momentum):
    start = momentum.astype(jnp.bfloat16)
    first = jnp.sum(jnp.square(start.astype(jnp.float32)))
    raw = block_gram(start)
    second = jnp.sum(raw * raw)
    ratio = SAFETY * (second + 1.0) / (first + 1.0)
    scale = lax.rsqrt(ratio)
    gram = (raw / ratio).astype(jnp.bfloat16)
    ymat = (jnp.dot(start, gram, preferred_element_type=jnp.float32) * scale).astype(jnp.bfloat16)
    zmat = jnp.dot(ymat, gram, preferred_element_type=jnp.float32).astype(jnp.bfloat16)
    current = (COEF_ONE * scale * start.astype(jnp.float32) + COEF_THREE * ymat.astype(jnp.float32) + COEF_FIVE * zmat.astype(jnp.float32)).astype(jnp.bfloat16)
    for index in range(ITERS - 1):
        gram = block_gram(current).astype(jnp.bfloat16)
        ymat = jnp.dot(current, gram, preferred_element_type=jnp.float32).astype(jnp.bfloat16)
        zmat = jnp.dot(ymat, gram, preferred_element_type=jnp.float32).astype(jnp.bfloat16)
        current = (COEF_ONE * current.astype(jnp.float32) + COEF_THREE * ymat.astype(jnp.float32) + COEF_FIVE * zmat.astype(jnp.float32)).astype(jnp.bfloat16)
    return current

def one_matrix(grads, velocity, weight):
    momentum = MOMENT * velocity + lax.optimization_barrier(jnp.sum(grads, axis=0))
    final = orthogonal(momentum)
    updated = SHRINK * weight - RATE * math.sqrt(weight.shape[0]) * final.astype(jnp.float32)
    return (momentum, updated)

def reference(gate_grads, gate_velocity, gate_weight, up_grads, up_velocity, up_weight, branch_grads, branch_velocity, branch_weight):
    gate_momentum, gate_updated = one_matrix(gate_grads, gate_velocity, gate_weight)
    up_momentum, up_updated = one_matrix(up_grads, up_velocity, up_weight)
    branch_momentum, branch_updated = one_matrix(branch_grads, branch_velocity, branch_weight)
    return (gate_momentum, gate_updated, up_momentum, up_updated, branch_momentum, branch_updated)
```

```python
import functools
import math

import jax
import jax.numpy as jnp
from jax import lax
from jax.experimental import pallas as pl
from jax.experimental.pallas import tpu as pltpu
from jax.sharding import PartitionSpec as P

MOMENT = 0.95
COEF_ONE = 3.4445
COEF_THREE = -4.775
COEF_FIVE = 2.0315
SAFETY = 2.0
RATE = 0.5
SHRINK = 0.95
STEP = 64
CHUNK = 176
GRANT = 67043328
F32 = jnp.float32
BF16 = jnp.bfloat16


def at(start, size, unit):
    return pl.ds(pl.multiple_of(start, unit), size)


def fit(rows, most):
    return max(n for n in range(16, most + 1, 16) if rows % n == 0)


def rows_loop(rows, most, body):
    step = fit(rows, most)

    def run(i, carry):
        body(at(i * step, step, step))
        return carry

    lax.fori_loop(0, rows // step, run, 0)


def kernel(nfs, ntp, *refs):
    (gg, gv, gw, ug, uv, uw, bg, bv, bw, gm, gu, um, uu, bm, bu) = refs[:15]
    (s, sb, vel, velb, gs, gsb, go, gob) = refs[15:23]
    (psend, part, prcv, rin, cross, tot, b0, b1, b2, gb) = refs[23:33]
    (c0, c1, c2, qs, qt, qtb, sums) = refs[33:40]
    (loc, rep_s, rep_r, ring_s, ring_r, half_s, half_r, in_s, in_r, mid_r) = refs[40:50]
    (out_s, out_r, ag_s, ag_r, dd_s, dd_r, gd_s, gd_r, pr_s, pr_r, q_s, q_r) = refs[50:62]

    height, size = s.shape[1:]
    width = size // ntp
    half = width // 2
    low, small = sb.shape
    thin = small // ntp
    count = 4
    tile = size // count

    f, t, r = lax.axis_index("fs"), lax.axis_index("tp"), lax.axis_index("rep")

    def turn(v):
        return v + v // 2 * (5 - 2 * v)

    p = turn(t)
    side = t % 2
    other = 1 - r
    peers = [turn((p + d) % ntp) for d in range(ntp)]
    across, beside, diagonal = t + 1 - 2 * side, (t + 2) % ntp, None
    diagonal = (across + 2) % ntp
    first_end, last_end = f == 0, f == nfs - 1
    is_end = jnp.logical_or(first_end, last_end)
    middle = nfs // 2
    is_mid = jnp.logical_or(f == middle - 1, f == middle)
    inward = jnp.where(f < middle, f + 1, f - 1)
    outward = jnp.where(f < middle, f - 1, f + 1)
    mate = {"rep": other}

    def send(src, dst, ssem, rsem, device):
        copy = pltpu.make_async_remote_copy(
            src_ref=src,
            dst_ref=dst,
            send_sem=ssem,
            recv_sem=rsem,
            device_id=device,
            device_id_type=pl.DeviceIdType.MESH,
        )
        return copy

    def arrived(dst, rsem):
        send(dst, dst, rsem, rsem, mate).wait_recv()

    def left(src, ssem):
        send(src, src, ssem, ssem, mate).wait_send()

    barrier = pltpu.get_barrier_semaphore()

    def greet(device):
        pl.semaphore_signal(
            barrier, inc=1, device_id=device, device_id_type=pl.DeviceIdType.MESH
        )

    grads, velocities, weights = (gg, ug, bg), (gv, uv, bv), (gw, uw, bw)
    outs_m, outs_u = (gm, um, bm), (gu, uu, bu)
    extents = ((height, width), (height, width), (low, thin))
    sent32 = (gs.at[0], gs.at[1], gsb)
    own32 = (go.at[0], go.at[1], gob)
    speed = (vel.at[0], vel.at[1], velb)
    txs = tuple(b1.at[:n, m * width : m * width + c] for m, (n, c) in enumerate(extents))
    rxs = tuple(b2.at[:n, m * width : m * width + c] for m, (n, c) in enumerate(extents))

    def local(src, dst, index):
        return pltpu.make_async_copy(src, dst, loc.at[index])

    loads = []
    for m in range(3):
        n = extents[m][0]
        loads.append(
            (
                local(grads[m].at[0, at(other * n, n, n)], sent32[m], m),
                local(grads[m].at[0, at(r * n, n, n)], own32[m], 3 + m),
                local(velocities[m], speed[m], 6 + m),
            )
        )
    for m in range(3):
        loads[m][0].start()
    for m in range(3):
        loads[m][1].start()
        loads[m][2].start()

    greet(mate)
    for d in range(1, ntp):
        greet({"tp": peers[d]})
    pl.when(f > 0)(lambda: greet({"fs": f - 1}))
    pl.when(f < nfs - 1)(lambda: greet({"fs": f + 1}))
    pl.semaphore_wait(barrier, ntp + jnp.minimum(f, 1) + jnp.minimum(nfs - 1 - f, 1))

    for m in range(3):
        loads[m][0].wait()

        def narrow(rows, m=m):
            txs[m][rows, :] = sent32[m][rows, :].astype(BF16)

        rows_loop(extents[m][0], STEP, narrow)
        send(txs[m], rxs[m], rep_s.at[m], rep_r.at[m], mate).start()

    mine = at(t * width, width, width)
    mine_b = at(t * thin, thin, thin)

    def ring(m, d):
        src = s.at[m, :, mine]
        send(src, src, ring_s.at[m, d], ring_r.at[m, d], {"tp": peers[d]}).start()

    def ring_b(d):
        src = sb.at[:, mine_b]
        send(src, src, ring_s.at[2, d], ring_r.at[2, d], {"tp": peers[d]}).start()

    def ring_in(m, d):
        spot = s.at[m, :, at(peers[ntp - d] * width, width, width)]
        arrived(spot, ring_r.at[m, d])

    def momentum(m):
        loads[m][1].wait()
        loads[m][2].wait()
        arrived(rxs[m], rep_r.at[m])

        def add(rows):
            total = own32[m][rows, :] + rxs[m][rows, :].astype(F32)
            value = MOMENT * speed[m][rows, :] + total
            speed[m][rows, :] = value
            if m < 2:
                s[m, rows, mine] = value.astype(BF16)
            else:
                sb[rows, mine_b] = value.astype(BF16)

        rows_loop(extents[m][0], STEP, add)
        local(speed[m], outs_m[m], 9 + m).start()

    def exchange(b, i, make):
        psend[b] = make(other)
        send(psend.at[b], prcv.at[b], half_s.at[i], half_r.at[i], mate).start()
        part[b] = make(r)

    def gram(slot, m, a, b):
        lo, hi = jnp.minimum(a, b), jnp.maximum(a, b)

        def make(h):
            return lax.dot_general(
                s[m, :, at(lo * width + h * half, half, half)],
                s[m, :, at(hi * width, width, width)],
                (((0,), (0,)), ((), ())),
                preferred_element_type=F32,
            ).astype(BF16)

        exchange(slot, slot, make)

    def add_into(b, ref):
        def add(rows):
            value = part[b, rows, :].astype(F32) + ref[rows, :].astype(F32)
            part[b, rows, :] = value.astype(BF16)

        rows_loop(half, STEP, add)

    def to_inner(b, i):
        send(part.at[b], rin.at[b], in_s.at[i], in_r.at[i], {"fs": inward}).start()

    def to_outer(b, i):
        send(tot.at[b], tot.at[b], out_s.at[i], out_r.at[i], {"fs": outward}).start()

    def chain_a(b, i):
        arrived(prcv.at[b], half_r.at[i])
        add_into(b, prcv.at[b])
        pl.when(jnp.logical_and(is_end, jnp.logical_not(is_mid)))(lambda: to_inner(b, i))

    def chain_b(b, i):
        @pl.when(jnp.logical_not(is_end))
        def _():
            arrived(rin.at[b], in_r.at[i])
            add_into(b, rin.at[b])
            pl.when(jnp.logical_not(is_mid))(lambda: to_inner(b, i))

        @pl.when(is_mid)
        def _():
            send(part.at[b], cross.at[i], in_s.at[i], mid_r.at[i], {"fs": inward}).start()

    def chain_c(b, i):
        @pl.when(is_mid)
        def _():
            arrived(cross.at[i], mid_r.at[i])

            def add(rows):
                value = part[b, rows, :].astype(F32) + cross[i, rows, :].astype(F32)
                tot[b, rows, :] = value.astype(BF16)

            rows_loop(half, STEP, add)
            pl.when(jnp.logical_not(is_end))(lambda: to_outer(b, i))

    def chain_d(b, i):
        @pl.when(jnp.logical_not(is_mid))
        def _():
            arrived(tot.at[b], out_r.at[i])
            pl.when(jnp.logical_not(is_end))(lambda: to_outer(b, i))

    def chain_end(b, i):
        left(psend.at[b], half_s.at[i])
        left(part.at[b], in_s.at[i])
        pl.when(jnp.logical_not(is_end))(lambda: left(tot.at[b], out_s.at[i]))

    def place(q, kind, matrix):
        a = turn(q)
        b = {
            0: a,
            1: turn((q + ntp - 1 + 2 * matrix) % ntp),
            2: turn((q + ntp // 2) % ntp),
        }[kind]
        return jnp.minimum(a, b), jnp.maximum(a, b)

    def spot(q, kind, matrix, h):
        i, j = place(q, kind, matrix)
        return b0.at[at(i * width + h * half, half, half), at(j * width, width, width)]

    kinds = (0, 1, 2, 0, 1, 0, 1, 2, 0, 1)
    owners = [p] * 3 + [turn(across)] * 2 + [turn(beside)] * 3 + [turn(diagonal)] * 2

    def gather_own(slot, kind, matrix):
        here = spot(p, kind, matrix, r)
        i, j = place(p, kind, matrix)

        def copy(rows):
            start = i * width + r * half
            b0[at(start + rows.start, STEP, STEP), at(j * width, width, width)] = tot[
                slot, rows, :
            ]

        rows_loop(half, STEP, copy)
        send(
            tot.at[slot], here, ag_s.at[slot, 0], ag_r.at[5 + kind], {"tp": beside}
        ).start()
        send(tot.at[slot], here, dd_s.at[kind], dd_r.at[kind], mate).start()

    def gather_far(slot, kind, matrix):
        here = spot(p, kind, matrix, r)
        send(
            tot.at[slot], here, ag_s.at[slot, 0], ag_r.at[3 + kind], {"tp": across}
        ).start()
        send(
            tot.at[slot], here, ag_s.at[slot, 1], ag_r.at[8 + kind], {"tp": diagonal}
        ).start()

    def gather(slot):
        if slot == 4:
            gather_own(slot, 2, side)
            return
        matrix, kind = slot // 2, slot % 2
        pl.when(side == matrix)(lambda: gather_own(slot, kind, matrix))
        pl.when(side != matrix)(lambda: gather_far(slot, kind, matrix))

    momentum(0)
    ring(0, 1)
    momentum(1)
    ring(1, ntp - 1)
    ring(1 - side, 2)
    gram(0, 0, t, t)
    gram(2, 1, t, t)
    momentum(2)
    chain_a(0, 0)
    chain_a(2, 2)
    chain_b(0, 0)
    chain_b(2, 2)
    ring_in(0, 1)
    gram(1, 0, peers[ntp - 1], t)
    ring_in(1, ntp - 1)
    gram(3, 1, peers[1], t)
    chain_a(1, 1)
    chain_a(3, 3)
    chain_c(0, 0)
    chain_c(2, 2)
    chain_b(1, 1)
    chain_b(3, 3)
    chain_d(0, 0)
    gather(0)
    chain_d(2, 2)
    gather(2)
    ring_in(side, 2)
    gram(4, side, peers[2], t)
    chain_a(4, 4)
    chain_c(1, 1)
    chain_c(3, 3)
    chain_b(4, 4)
    chain_d(1, 1)
    gather(1)
    chain_d(3, 3)
    gather(3)
    chain_c(4, 4)
    chain_d(4, 4)
    gather(4)

    for m in range(3):
        left(txs[m], rep_s.at[m])
    for e in (3, 5, 8, 4, 6, 9, 7):
        here = spot(owners[e], kinds[e], side, r)
        arrived(here, ag_r.at[e])
        send(here, here, dd_s.at[e], dd_r.at[e], mate).start()

    sums[...] = jnp.zeros_like(sums)

    def fold(value):
        return jnp.sum(value.reshape(-1, 8, value.shape[1]), axis=0)

    def survey(ref, i, j, diag, span):
        def add(rows):
            wide = ref[at(i + rows.start, STEP, STEP), at(j, span, span)].astype(F32)
            weight = 1.0 if diag else 2.0
            sums[1, :, :span] += weight * fold(wide * wide)
            if diag:
                down = lax.broadcasted_iota(jnp.int32, wide.shape, 0) + rows.start
                over = lax.broadcasted_iota(jnp.int32, wide.shape, 1)
                sums[0, :, :span] += fold(jnp.where(down == over, wide, 0.0))

        rows_loop(span, STEP, add)

    def scales():
        first = jnp.sum(jnp.sum(sums[0], axis=0, keepdims=True), axis=1, keepdims=True)
        second = jnp.sum(jnp.sum(sums[1], axis=0, keepdims=True), axis=1, keepdims=True)
        ratio = SAFETY * (second + 1.0) / (first + 1.0)
        return 1.0 / ratio, lax.rsqrt(ratio)

    for e in range(10):
        arrived(spot(owners[e], kinds[e], side, other), dd_r.at[e])
        i, j = place(owners[e], kinds[e], side)
        survey(b0, i * width, j * width, kinds[e] == 0, width)
        if kinds[e] != 0:
            b0[at(j * width, width, width), at(i * width, width, width)] = b0[
                at(i * width, width, width), at(j * width, width, width)
            ].T

    for slot in range(5):
        left(tot.at[slot], ag_s.at[slot, 0])
        if slot < 4:
            pl.when(side != slot // 2)(lambda slot=slot: left(tot.at[slot], ag_s.at[slot, 1]))
        chain_end(slot, slot)
    for e in range(10):
        left(tot.at[0], dd_s.at[e])
    ring(0, ntp - 1)
    ring(1, 1)
    ring(side, 2)
    for d in range(1, ntp):
        ring_b(d)
    for m in range(3):
        local(speed[m], outs_m[m], 9 + m).wait()
        local(weights[m], speed[m], 12 + m).start()

    inverse, scale = scales()

    def eye(shape, shift):
        down = lax.broadcasted_iota(jnp.int32, shape, 0)
        over = lax.broadcasted_iota(jnp.int32, shape, 1)
        return jnp.where(down == over + shift, COEF_ONE, 0.0)

    def product(index, lhs, rhs, out, finish):
        def where(k, who):
            third, fourth = k // 3, k // 4
            i, j = third - fourth, k - 2 * third + fourth
            i, j = (
                i + who * (3 - j + fourth - i),
                j + who * (3 - i - fourth - j),
            )
            return i, j

        def step(k, carry):
            i, j = where(k, r)
            rows, cols = at(i * tile, tile, tile), at(j * tile, tile, tile)
            acc = jnp.dot(lhs[rows, :], rhs[:, cols], preferred_element_type=F32)
            value = finish(acc, lhs, rows, cols, (j - i) * tile).astype(BF16)
            out[rows, cols] = value
            here = out.at[rows, cols]
            send(here, here, pr_s.at[index, k], pr_r.at[index, k], mate).start()

            @pl.when(i != j)
            def _():
                out[cols, rows] = value.T

            return carry

        lax.fori_loop(0, 5, step, 0)

        def take(k, carry):
            i, j = where(k, other)
            rows, cols = at(i * tile, tile, tile), at(j * tile, tile, tile)
            here = out.at[rows, cols]
            arrived(here, pr_r.at[index, k])

            @pl.when(i != j)
            def _():
                out[cols, rows] = out[rows, cols].T

            left(here, pr_s.at[index, k])
            return carry

        lax.fori_loop(0, 5, take, 0)

    def poly_one(inv):
        def finish(acc, lhs, rows, cols, shift):
            gram_part = lhs[rows, cols].astype(F32) * inv
            return eye(acc.shape, shift) + COEF_THREE * gram_part + COEF_FIVE * (acc * inv * inv)

        return finish

    def times(inv):
        return lambda acc, lhs, rows, cols, shift: acc * inv

    def plain(acc, lhs, rows, cols, shift):
        return acc

    def poly_two(acc, lhs, rows, cols, shift):
        return eye(acc.shape, shift) + COEF_THREE * lhs[rows, cols].astype(F32) + COEF_FIVE * acc

    product(0, b0, b0, b1, poly_one(inverse))

    for d in range(1, ntp):
        arrived(sb.at[:, at(peers[ntp - d] * thin, thin, thin)], ring_r.at[2, d])
    deep, wide_b = small // 2 // half, small // width
    blocks = deep * wide_b
    for b in range(blocks):
        def make(h, b=b):
            return lax.dot_general(
                sb[:, at(h * (small // 2) + b // wide_b * half, half, half)],
                sb[:, b % wide_b * width : (b % wide_b + 1) * width],
                (((0,), (0,)), ((), ())),
                preferred_element_type=F32,
            ).astype(BF16)

        exchange(b, 5 + b, make)
    product(1, b0, b1, b2, times(inverse))
    for b in range(blocks):
        chain_a(b, 5 + b)
    product(2, b2, b1, b0, plain)
    for b in range(blocks):
        chain_b(b, 5 + b)
    product(3, b0, b0, b2, poly_two)
    for b in range(blocks):
        chain_c(b, 5 + b)

    def panel(lhs, rhs, out, span, finish):
        def step(j, carry):
            cols = at(j * tile, tile, tile)
            acc = jnp.dot(lhs(), rhs(cols), preferred_element_type=F32)
            out(cols, finish(acc, cols).astype(BF16))
            return carry

        lax.fori_loop(0, span // tile, step, 0)

    def same(acc, cols):
        return acc

    def factor(begin, g2, p1, p2, span, scaling, out):
        def buf(ref):
            return lambda: ref[:, :span]

        def put(ref):
            def write(cols, value):
                ref[:, cols] = value

            return write

        def cubic(acc, cols):
            shift = cols.start - begin
            return (
                eye(acc.shape, shift)
                + COEF_THREE * c1[:, cols].astype(F32)
                + COEF_FIVE * acc
            )

        panel(lambda: p2(at(begin, half, half), None), lambda c: p2(None, c), put(c0), span, same)
        panel(buf(c0), lambda c: g2(None, c), put(c1), span, same)
        panel(buf(c1), lambda c: g2(None, c), put(c2), span, same)
        panel(buf(c2), lambda c: p2(None, c), put(c0), span, same)
        panel(buf(c0), lambda c: p2(None, c), put(c2), span, cubic)
        panel(buf(c2), lambda c: p2(None, c), put(c0), span, same)
        panel(buf(c0), lambda c: p1(None, c), out, span, lambda acc, cols: acc * scaling)

    def view(ref, top, span):
        def read(rows, cols):
            if rows is None:
                return ref[top : top + span, cols]
            return ref[at(top + rows.start, half, half), :span]

        return read

    big = (view(b0, 0, size), view(b1, 0, size), view(b2, 0, size))

    def put_qs(cols, value):
        qs[:, cols] = value

    def put_qt(cols, value):
        qt[side, at(r * half, half, half), cols] = value

    def put_qb(cols, value):
        qtb[:, cols] = value

    factor(across * width + r * half, *big, size, scale, put_qs)
    landing = qt.at[side, at(r * half, half, half)]
    send(qs, landing, q_s.at[0], q_r.at[0], {"tp": across}).start()
    for b in range(blocks):
        chain_d(b, 5 + b)
        a, c = b // wide_b, b % wide_b
        start = r * (small // 2) + a * half
        here = gb.at[at(start, half, half), c * width : (c + 1) * width]

        def copy(rows, b=b, start=start, c=c):
            gb[at(start + rows.start, STEP, STEP), c * width : (c + 1) * width] = tot[b, rows, :]

        rows_loop(half, STEP, copy)
        send(tot.at[b], here, gd_s.at[b], gd_r.at[b], mate).start()
    factor(t * width + r * half, *big, size, scale, put_qt)
    send(landing, landing, q_s.at[1], q_r.at[1], mate).start()

    for b in range(blocks):
        a, c = b // wide_b, b % wide_b
        start = other * (small // 2) + a * half
        arrived(gb.at[at(start, half, half), c * width : (c + 1) * width], gd_r.at[b])
    sums[...] = jnp.zeros_like(sums)
    for i in range(0, small, width):
        for j in range(0, small, width):
            if i == j:
                survey(gb, i, j, True, width)
            if i < j:
                survey(gb, i, j, False, width)
    inverse_b, scale_b = scales()

    def square(lhs, rhs, out, finish):
        def step(n, carry):
            i, j = n // (small // tile), n % (small // tile)
            rows, cols = at(i * tile, tile, tile), at(j * tile, tile, tile)
            acc = jnp.dot(lhs[rows, :small], rhs[:small, cols], preferred_element_type=F32)
            out[rows, cols] = finish(acc, lhs, rows, cols, (j - i) * tile).astype(BF16)
            return carry

        lax.fori_loop(0, (small // tile) ** 2, step, 0)

    square(gb, gb, b1, poly_one(inverse_b))
    square(gb, b1, b2, times(inverse_b))
    square(b2, b1, b0, plain)
    square(b0, b0, b2, poly_two)
    tiny = (view(b0, 0, small), view(b1, 0, small), view(b2, 0, small))
    factor(t * thin, *tiny, small, scale_b, put_qb)

    def update(m, lhs, rhs, rate, ref, rows_of, step):
        def body(rows):
            acc = lax.dot_general(
                lhs(rows), rhs(), (((1,), (1,)), ((), ())), preferred_element_type=F32
            )
            ref(rows, acc, rate)

        rows_loop(rows_of, step, body)

    def put_big(m):
        def write(rows, acc, rate):
            vel[m, rows, :] = SHRINK * vel[m, rows, :] - rate * acc

        return write

    def put_small(rows, acc, rate):
        velb[rows, :] = SHRINK * velb[rows, :] - rate * acc

    rate = RATE * math.sqrt(height * nfs * 2)
    rate_b = RATE * math.sqrt(low * nfs * 2)

    def finish_big(m):
        update(m, lambda rows: s[m, rows, :], lambda: qt[m], rate, put_big(m), height, CHUNK)

        @pl.when(m == 0)
        def _():
            local(speed[0], gu, 15).start()

        @pl.when(m == 1)
        def _():
            local(speed[1], uu, 16).start()

    for m in range(3):
        local(weights[m], speed[m], 12 + m).wait()
    update(2, lambda rows: sb[rows, :], lambda: qtb[...], rate_b, put_small, low, CHUNK)
    local(velb, bu, 17).start()
    ring_in(0, ntp - 1)
    ring_in(1, 1)
    ring_in(1 - side, 2)
    arrived(qt.at[side, at(other * half, half, half)], q_r.at[1])
    finish_big(side)
    far = qt.at[1 - side, at(r * half, half, half)]
    arrived(far, q_r.at[0])
    send(far, far, q_s.at[2], q_r.at[2], mate).start()
    arrived(qt.at[1 - side, at(other * half, half, half)], q_r.at[2])
    finish_big(1 - side)

    for m in range(3):
        for d in range(1, ntp):
            block = s.at[m, :, mine] if m < 2 else sb.at[:, mine_b]
            left(block, ring_s.at[m, d])
    for b in range(blocks):
        chain_end(b, 5 + b)
        left(tot.at[b], gd_s.at[b])
    left(qs, q_s.at[0])
    left(landing, q_s.at[1])
    left(far, q_s.at[2])
    local(speed[0], gu, 15).wait()
    local(speed[1], uu, 16).wait()
    local(velb, bu, 17).wait()


def local_part(nfs, ntp, *args):
    height, width = args[1].shape
    low, thin = args[7].shape
    size, small = width * ntp, thin * ntp
    half = width // 2
    blocks = small // 2 // half * (small // width)
    vmem = pltpu.VMEM
    dma = pltpu.SemaphoreType.DMA
    scratch = [
        vmem((2, height, size), BF16),
        vmem((low, small), BF16),
        vmem((2, height, width), F32),
        vmem((low, thin), F32),
        vmem((2, height, width), F32),
        vmem((low, thin), F32),
        vmem((2, height, width), F32),
        vmem((low, thin), F32),
    ]
    scratch += [vmem((5, half, width), BF16)] * 4
    scratch += [vmem((5 + blocks, half, width), BF16), vmem((5, half, width), BF16)]
    scratch += [vmem((size, size), BF16)] * 3 + [vmem((small, small), BF16)]
    scratch += [vmem((half, size), BF16)] * 4
    scratch += [vmem((2, width, size), BF16), vmem((thin, small), BF16), vmem((2, 8, width), F32)]
    slots = dma((5 + blocks,))
    scratch += [dma((18,)), dma((3,)), dma((3,)), dma((3, ntp)), dma((3, ntp))]
    scratch += [slots] * 7
    scratch += [dma((5, 2)), dma((10,)), dma((10,)), dma((10,)), dma((blocks,)), dma((blocks,))]
    scratch += [dma((4, 5)), dma((4, 5)), dma((3,)), dma((3,))]
    outs = []
    for i in range(3):
        outs += [jax.ShapeDtypeStruct(args[3 * i + 1].shape, F32)] * 2
    return pl.pallas_call(
        functools.partial(kernel, nfs, ntp),
        out_shape=tuple(outs),
        in_specs=[pl.BlockSpec(memory_space=pl.ANY)] * 9,
        out_specs=tuple([pl.BlockSpec(memory_space=pl.ANY)] * 6),
        scratch_shapes=scratch,
        compiler_params=pltpu.CompilerParams(
            collective_id=0, has_side_effects=True, vmem_limit_bytes=GRANT
        ),
        name="orthogonal",
    )(*args)


def solution(mesh):
    sizes = mesh.shape
    split = P(("fs", "rep"), "tp")
    return jax.shard_map(
        functools.partial(local_part, sizes["fs"], sizes["tp"]),
        mesh=mesh,
        in_specs=(P("rep", "fs", "tp"), split, split) * 3,
        out_specs=(split,) * 6,
        check_vma=False,
    )
```

```python
import functools
import math

import jax
import jax.numpy as jnp
from jax import lax
from jax.experimental import pallas as pl
from jax.experimental.pallas import tpu as pltpu
from jax.sharding import PartitionSpec as P

MOMENT = 0.95
COEF_ONE = 3.4445
COEF_THREE = -4.775
COEF_FIVE = 2.0315
SAFETY = 2.0
RATE = 0.5
SHRINK = 0.95
STEP = 64
CHUNK = 176
GRANT = 67043328
F32 = jnp.float32
BF16 = jnp.bfloat16


def at(start, size, unit):
    return pl.ds(pl.multiple_of(start, unit), size)


def fit(rows, most):
    return max(n for n in range(16, most + 1, 16) if rows % n == 0)


def rows_loop(rows, most, body):
    step = fit(rows, most)

    def run(i, carry):
        body(at(i * step, step, step))
        return carry

    lax.fori_loop(0, rows // step, run, 0)


def kernel(nfs, ntp, *refs):
    (gg, gv, gw, ug, uv, uw, bg, bv, bw, gm, gu, um, uu, bm, bu) = refs[:15]
    (s, sb, vel, velb, gs, gsb, go, gob) = refs[15:23]
    (psend, part, prcv, rin, cross, tot, b0, b1, b2, gb) = refs[23:33]
    (c0, c1, c2, qs, qt, qtb, sums) = refs[33:40]
    (loc, rep_s, rep_r, ring_s, ring_r, half_s, half_r, in_s, in_r, mid_r) = refs[40:50]
    (out_s, out_r, ag_s, ag_r, dd_s, dd_r, gd_s, gd_r, pr_s, pr_r, q_s, q_r) = refs[50:62]
    (x_s, x_r, st_s, st_r, sd_s, sd_r) = refs[62:68]

    height, size = s.shape[1:]
    width = size // ntp
    half = width // 2
    low, small = sb.shape
    thin = small // ntp
    count = 4
    tile = size // count

    f, t, r = lax.axis_index("fs"), lax.axis_index("tp"), lax.axis_index("rep")

    def turn(v):
        return v + v // 2 * (5 - 2 * v)

    p = turn(t)
    side = t % 2
    other = 1 - r
    peers = [turn((p + d) % ntp) for d in range(ntp)]
    across, beside, diagonal = t + 1 - 2 * side, (t + 2) % ntp, None
    diagonal = (across + 2) % ntp
    first_end, last_end = f == 0, f == nfs - 1
    is_end = jnp.logical_or(first_end, last_end)
    middle = nfs // 2
    is_mid = jnp.logical_or(f == middle - 1, f == middle)
    inward = jnp.where(f < middle, f + 1, f - 1)
    outward = jnp.where(f < middle, f - 1, f + 1)
    mate = {"rep": other}

    def send(src, dst, ssem, rsem, device):
        copy = pltpu.make_async_remote_copy(
            src_ref=src,
            dst_ref=dst,
            send_sem=ssem,
            recv_sem=rsem,
            device_id=device,
            device_id_type=pl.DeviceIdType.MESH,
        )
        return copy

    def arrived(dst, rsem):
        send(dst, dst, rsem, rsem, mate).wait_recv()

    def left(src, ssem):
        send(src, src, ssem, ssem, mate).wait_send()

    barrier = pltpu.get_barrier_semaphore()

    def greet(device):
        pl.semaphore_signal(
            barrier, inc=1, device_id=device, device_id_type=pl.DeviceIdType.MESH
        )

    grads, velocities, weights = (gg, ug, bg), (gv, uv, bv), (gw, uw, bw)
    outs_m, outs_u = (gm, um, bm), (gu, uu, bu)
    extents = ((height, width), (height, width), (low, thin))
    sent32 = (gs.at[0], gs.at[1], gsb)
    own32 = (go.at[0], go.at[1], gob)
    speed = (vel.at[0], vel.at[1], velb)
    txs = tuple(b1.at[:n, m * width : m * width + c] for m, (n, c) in enumerate(extents))
    rxs = tuple(b2.at[:n, m * width : m * width + c] for m, (n, c) in enumerate(extents))

    def local(src, dst, index):
        return pltpu.make_async_copy(src, dst, loc.at[index])

    loads = []
    for m in range(3):
        n = extents[m][0]
        loads.append(
            (
                local(grads[m].at[0, at(other * n, n, n)], sent32[m], m),
                local(grads[m].at[0, at(r * n, n, n)], own32[m], 3 + m),
                local(velocities[m], speed[m], 6 + m),
            )
        )
    for m in range(3):
        loads[m][0].start()
    for m in range(3):
        loads[m][1].start()
        loads[m][2].start()

    greet(mate)
    for d in range(1, ntp):
        greet({"tp": peers[d]})
    pl.when(f > 0)(lambda: greet({"fs": f - 1}))
    pl.when(f < nfs - 1)(lambda: greet({"fs": f + 1}))
    pl.semaphore_wait(barrier, ntp + jnp.minimum(f, 1) + jnp.minimum(nfs - 1 - f, 1))

    for m in range(3):
        loads[m][0].wait()

        def narrow(rows, m=m):
            txs[m][rows, :] = sent32[m][rows, :].astype(BF16)

        rows_loop(extents[m][0], STEP, narrow)
        send(txs[m], rxs[m], rep_s.at[m], rep_r.at[m], mate).start()

    mine = at(t * width, width, width)
    mine_b = at(t * thin, thin, thin)

    def ring(m, d):
        src = s.at[m, :, mine]
        send(src, src, ring_s.at[m, d], ring_r.at[m, d], {"tp": peers[d]}).start()

    def ring_b(d):
        src = sb.at[:, mine_b]
        send(src, src, ring_s.at[2, d], ring_r.at[2, d], {"tp": peers[d]}).start()

    def ring_in(m, d):
        spot = s.at[m, :, at(peers[ntp - d] * width, width, width)]
        arrived(spot, ring_r.at[m, d])

    def momentum(m):
        loads[m][1].wait()
        loads[m][2].wait()
        arrived(rxs[m], rep_r.at[m])

        def add(rows):
            total = own32[m][rows, :] + rxs[m][rows, :].astype(F32)
            value = MOMENT * speed[m][rows, :] + total
            speed[m][rows, :] = value
            if m < 2:
                s[m, rows, mine] = value.astype(BF16)
            else:
                sb[rows, mine_b] = value.astype(BF16)

        rows_loop(extents[m][0], STEP, add)
        local(speed[m], outs_m[m], 9 + m).start()

    def exchange(b, i, make):
        psend[b] = make(other)
        send(psend.at[b], prcv.at[b], half_s.at[i], half_r.at[i], mate).start()
        part[b] = make(r)

    def gram(slot, m, a, b):
        lo, hi = jnp.minimum(a, b), jnp.maximum(a, b)

        def make(h):
            return lax.dot_general(
                s[m, :, at(lo * width + h * half, half, half)],
                s[m, :, at(hi * width, width, width)],
                (((0,), (0,)), ((), ())),
                preferred_element_type=F32,
            ).astype(BF16)

        exchange(slot, slot, make)

    def add_into(b, ref):
        def add(rows):
            value = part[b, rows, :].astype(F32) + ref[rows, :].astype(F32)
            part[b, rows, :] = value.astype(BF16)

        rows_loop(half, STEP, add)

    def to_inner(b, i):
        send(part.at[b], rin.at[b], in_s.at[i], in_r.at[i], {"fs": inward}).start()

    def to_outer(b, i):
        send(tot.at[b], tot.at[b], out_s.at[i], out_r.at[i], {"fs": outward}).start()

    def chain_a(b, i):
        arrived(prcv.at[b], half_r.at[i])
        add_into(b, prcv.at[b])
        pl.when(jnp.logical_and(is_end, jnp.logical_not(is_mid)))(lambda: to_inner(b, i))

    def chain_b(b, i):
        @pl.when(jnp.logical_not(is_end))
        def _():
            arrived(rin.at[b], in_r.at[i])
            add_into(b, rin.at[b])
            pl.when(jnp.logical_not(is_mid))(lambda: to_inner(b, i))

        @pl.when(is_mid)
        def _():
            send(part.at[b], cross.at[i], in_s.at[i], mid_r.at[i], {"fs": inward}).start()

    def chain_c(b, i):
        @pl.when(is_mid)
        def _():
            arrived(cross.at[i], mid_r.at[i])

            def add(rows):
                value = part[b, rows, :].astype(F32) + cross[i, rows, :].astype(F32)
                tot[b, rows, :] = value.astype(BF16)

            rows_loop(half, STEP, add)
            pl.when(jnp.logical_not(is_end))(lambda: to_outer(b, i))

    def chain_d(b, i):
        @pl.when(jnp.logical_not(is_mid))
        def _():
            arrived(tot.at[b], out_r.at[i])
            pl.when(jnp.logical_not(is_end))(lambda: to_outer(b, i))

    def chain_end(b, i):
        left(psend.at[b], half_s.at[i])
        left(part.at[b], in_s.at[i])
        pl.when(jnp.logical_not(is_end))(lambda: left(tot.at[b], out_s.at[i]))

    def place(q, kind, matrix):
        a = turn(q)
        b = {
            0: a,
            1: turn((q + ntp - 1 + 2 * matrix) % ntp),
            2: turn((q + ntp // 2) % ntp),
        }[kind]
        return jnp.minimum(a, b), jnp.maximum(a, b)

    def spot(q, kind, matrix, h):
        i, j = place(q, kind, matrix)
        return b0.at[at(i * width + h * half, half, half), at(j * width, width, width)]

    kinds = (0, 1, 2, 0, 1, 0, 1, 2, 0, 1)
    owners = [p] * 3 + [turn(across)] * 2 + [turn(beside)] * 3 + [turn(diagonal)] * 2

    def gather_own(slot, kind, matrix):
        here = spot(p, kind, matrix, r)
        i, j = place(p, kind, matrix)

        def copy(rows):
            start = i * width + r * half
            b0[at(start + rows.start, STEP, STEP), at(j * width, width, width)] = tot[
                slot, rows, :
            ]

        rows_loop(half, STEP, copy)
        send(
            tot.at[slot], here, ag_s.at[slot, 0], ag_r.at[5 + kind], {"tp": beside}
        ).start()
        send(tot.at[slot], here, dd_s.at[kind], dd_r.at[kind], mate).start()

    def gather_far(slot, kind, matrix):
        here = spot(p, kind, matrix, r)
        send(
            tot.at[slot], here, ag_s.at[slot, 0], ag_r.at[3 + kind], {"tp": across}
        ).start()
        send(
            tot.at[slot], here, ag_s.at[slot, 1], ag_r.at[8 + kind], {"tp": diagonal}
        ).start()

    def gather(slot):
        if slot == 4:
            gather_own(slot, 2, side)
            return
        matrix, kind = slot // 2, slot % 2
        pl.when(side == matrix)(lambda: gather_own(slot, kind, matrix))
        pl.when(side != matrix)(lambda: gather_far(slot, kind, matrix))

    momentum(0)
    ring(0, 1)
    momentum(1)
    ring(1, ntp - 1)
    ring(1 - side, 2)
    gram(0, 0, t, t)
    gram(2, 1, t, t)
    momentum(2)
    chain_a(0, 0)
    chain_a(2, 2)
    chain_b(0, 0)
    chain_b(2, 2)
    ring_in(0, 1)
    gram(1, 0, peers[ntp - 1], t)
    ring_in(1, ntp - 1)
    gram(3, 1, peers[1], t)
    chain_a(1, 1)
    chain_a(3, 3)
    chain_c(0, 0)
    chain_c(2, 2)
    chain_b(1, 1)
    chain_b(3, 3)
    chain_d(0, 0)
    gather(0)
    chain_d(2, 2)
    gather(2)
    ring_in(side, 2)
    gram(4, side, peers[2], t)
    chain_a(4, 4)
    chain_c(1, 1)
    chain_c(3, 3)
    chain_b(4, 4)
    chain_d(1, 1)
    gather(1)
    chain_d(3, 3)
    gather(3)
    chain_c(4, 4)
    chain_d(4, 4)
    gather(4)

    for m in range(3):
        left(txs[m], rep_s.at[m])
    for d in range(1, ntp):
        ring_b(d)
    for e in (3, 5, 8, 4, 6, 9, 7):
        here = spot(owners[e], kinds[e], side, r)
        arrived(here, ag_r.at[e])
        send(here, here, dd_s.at[e], dd_r.at[e], mate).start()

    sums[...] = jnp.zeros_like(sums)

    def fold(value):
        return jnp.sum(value.reshape(-1, 8, value.shape[1]), axis=0)

    def survey(ref, i, j, diag, span):
        def add(rows):
            wide = ref[at(i + rows.start, STEP, STEP), at(j, span, span)].astype(F32)
            weight = 1.0 if diag else 2.0
            sums[1, :, :span] += weight * fold(wide * wide)
            if diag:
                down = lax.broadcasted_iota(jnp.int32, wide.shape, 0) + rows.start
                over = lax.broadcasted_iota(jnp.int32, wide.shape, 1)
                sums[0, :, :span] += fold(jnp.where(down == over, wide, 0.0))

        rows_loop(span, STEP, add)

    def scales():
        first = jnp.sum(jnp.sum(sums[0], axis=0, keepdims=True), axis=1, keepdims=True)
        second = jnp.sum(jnp.sum(sums[1], axis=0, keepdims=True), axis=1, keepdims=True)
        ratio = SAFETY * (second + 1.0) / (first + 1.0)
        return 1.0 / ratio, lax.rsqrt(ratio)

    for e in range(10):
        arrived(spot(owners[e], kinds[e], side, other), dd_r.at[e])
        i, j = place(owners[e], kinds[e], side)
        survey(b0, i * width, j * width, kinds[e] == 0, width)
        if kinds[e] != 0:
            b0[at(j * width, width, width), at(i * width, width, width)] = b0[
                at(i * width, width, width), at(j * width, width, width)
            ].T

    for slot in range(5):
        left(tot.at[slot], ag_s.at[slot, 0])
        if slot < 4:
            pl.when(side != slot // 2)(lambda slot=slot: left(tot.at[slot], ag_s.at[slot, 1]))
        chain_end(slot, slot)
    for e in range(10):
        left(tot.at[0], dd_s.at[e])
    ring(0, ntp - 1)
    ring(1, 1)
    ring(side, 2)
    for m in range(3):
        local(speed[m], outs_m[m], 9 + m).wait()
        local(weights[m], speed[m], 12 + m).start()

    inverse, scale = scales()

    def eye(shape, shift):
        down = lax.broadcasted_iota(jnp.int32, shape, 0)
        over = lax.broadcasted_iota(jnp.int32, shape, 1)
        return jnp.where(down == over + shift, COEF_ONE, 0.0)

    def product(index, lhs, rhs, out, finish):
        def where(k, who):
            third, fourth = k // 3, k // 4
            i, j = third - fourth, k - 2 * third + fourth
            i, j = (
                i + who * (3 - j + fourth - i),
                j + who * (3 - i - fourth - j),
            )
            return i, j

        def step(k, carry):
            i, j = where(k, r)
            rows, cols = at(i * tile, tile, tile), at(j * tile, tile, tile)
            acc = jnp.dot(lhs[rows, :], rhs[:, cols], preferred_element_type=F32)
            value = finish(acc, lhs, rows, cols, (j - i) * tile).astype(BF16)
            out[rows, cols] = value
            here = out.at[rows, cols]
            send(here, here, pr_s.at[index, k], pr_r.at[index, k], mate).start()

            @pl.when(i != j)
            def _():
                out[cols, rows] = value.T

            return carry

        lax.fori_loop(0, 5, step, 0)

        def take(k, carry):
            i, j = where(k, other)
            rows, cols = at(i * tile, tile, tile), at(j * tile, tile, tile)
            here = out.at[rows, cols]
            arrived(here, pr_r.at[index, k])

            @pl.when(i != j)
            def _():
                out[cols, rows] = out[rows, cols].T

            left(here, pr_s.at[index, k])
            return carry

        lax.fori_loop(0, 5, take, 0)

    def poly_one(inv):
        def finish(acc, lhs, rows, cols, shift):
            gram_part = lhs[rows, cols].astype(F32) * inv
            return eye(acc.shape, shift) + COEF_THREE * gram_part + COEF_FIVE * (acc * inv * inv)

        return finish

    def times(inv):
        return lambda acc, lhs, rows, cols, shift: acc * inv

    def plain(acc, lhs, rows, cols, shift):
        return acc

    def poly_two(acc, lhs, rows, cols, shift):
        return eye(acc.shape, shift) + COEF_THREE * lhs[rows, cols].astype(F32) + COEF_FIVE * acc

    for d in range(1, ntp):
        arrived(sb.at[:, at(peers[ntp - d] * thin, thin, thin)], ring_r.at[2, d])
    deep, wide_b = small // 2 // half, small // width
    blocks = deep * wide_b
    for b in range(blocks):
        def make(h, b=b):
            return lax.dot_general(
                sb[:, at(h * (small // 2) + b // wide_b * half, half, half)],
                sb[:, b % wide_b * width : (b % wide_b + 1) * width],
                (((0,), (0,)), ((), ())),
                preferred_element_type=F32,
            ).astype(BF16)

        exchange(b, 5 + b, make)
    product(0, b0, b0, b1, poly_one(inverse))

    for b in range(blocks):
        chain_a(b, 5 + b)
    product(1, b0, b1, b2, times(inverse))
    chain_b(0, 5)
    product(2, b2, b1, b0, plain)
    chain_b(1, 6)
    chain_c(0, 5)
    product(3, b0, b0, b2, poly_two)
    chain_b(2, 7)
    chain_b(3, 8)
    chain_c(1, 6)

    def panel(lhs, rhs, out, span, finish):
        def step(j, carry):
            cols = at(j * tile, tile, tile)
            acc = jnp.dot(lhs(), rhs(cols), preferred_element_type=F32)
            out(cols, finish(acc, cols).astype(BF16))
            return carry

        lax.fori_loop(0, span // tile, step, 0)

    def same(acc, cols):
        return acc

    def factor(rows, begin, extra, g2, p1, p2, span, scaling, out, tasks):
        def buf(ref):
            return lambda: ref[:rows, :span]

        def put(ref):
            def write(cols, value):
                ref[:rows, cols] = value

            return write

        def cubic(acc, cols):
            down = lax.broadcasted_iota(jnp.int32, acc.shape, 0)
            over = lax.broadcasted_iota(jnp.int32, acc.shape, 1)
            down = down + jnp.where(down < half, begin, extra - half)
            unit = jnp.where(down == over + cols.start, COEF_ONE, 0.0)
            return unit + COEF_THREE * c1[:rows, cols].astype(F32) + COEF_FIVE * acc

        panel(buf(c2), p2, put(c0), span, same)
        tasks(0)
        panel(buf(c0), g2, put(c1), span, same)
        tasks(1)
        panel(buf(c1), g2, put(c2), span, same)
        tasks(2)
        panel(buf(c2), p2, put(c0), span, same)
        tasks(3)
        panel(buf(c0), p2, put(c2), span, cubic)
        tasks(4)
        panel(buf(c2), p2, put(c0), span, same)
        tasks(5)
        panel(buf(c0), p1, out, span, lambda acc, cols: acc * scaling)

    def view(ref, top, span):
        return lambda cols: ref[top : top + span, cols]

    slab = half // nfs
    begin, extra = t * width + r * half, across * width + r * half + f * slab

    def put_q(cols, value):
        qt[side, at(r * half, half, half), cols] = value[:half]
        qs[:, cols] = value[half:]

    def put_qb(cols, value):
        qtb[:, cols] = value

    def fill(rows):
        c2[rows, :] = b2[at(begin + rows.start, STEP, STEP), :]

    rows_loop(half, STEP, fill)
    c2[half : half + slab, :] = b2[at(extra, slab, slab), :]

    def tasks(n):
        if n == 1:
            chain_c(2, 7)
        if n == 3:
            chain_c(3, 8)

    factor(
        half + slab, begin, extra, view(b0, 0, size), view(b1, 0, size), view(b2, 0, size),
        size, scale, put_q, tasks,
    )

    def strip(m, who, j):
        return qt.at[m, at(who * half + j * slab, slab, slab)]

    send(qs, strip(side, r, f), x_s, x_r, {"tp": across}).start()
    landing = qt.at[side, at(r * half, half, half)]
    send(landing, landing, q_s, q_r, mate).start()
    for b in range(blocks):
        chain_d(b, 5 + b)
        a, c = b // wide_b, b % wide_b
        start = r * (small // 2) + a * half
        here = gb.at[at(start, half, half), c * width : (c + 1) * width]

        def copy(rows, b=b, start=start, c=c):
            gb[at(start + rows.start, STEP, STEP), c * width : (c + 1) * width] = tot[b, rows, :]

        rows_loop(half, STEP, copy)
        send(tot.at[b], here, gd_s.at[b], gd_r.at[b], mate).start()

    def pass_on(d, up):
        here = strip(1 - side, r, f)
        from_far = d > 0
        j = f - d if up else f + d
        ahead = f + 1 if up else f - 1
        inside = jnp.logical_and(j >= 0, j < nfs)
        more = jnp.logical_and(ahead >= 0, ahead < nfs)
        lane = 0 if up else 1
        if from_far:
            @pl.when(inside)
            def _():
                spot = strip(1 - side, r, j)
                arrived(spot, st_r.at[lane, d])
                send(spot, spot, sd_s.at[lane, d], sd_r.at[lane, d], mate).start()

                @pl.when(more)
                def _():
                    send(
                        spot, spot, st_s.at[lane, d], st_r.at[lane, d + 1], {"fs": ahead}
                    ).start()
        else:
            @pl.when(more)
            def _():
                send(here, here, st_s.at[lane, 0], st_r.at[lane, 1], {"fs": ahead}).start()

    def travel(d):
        if d == 0:
            here = strip(1 - side, r, f)
            arrived(here, x_r)
            pass_on(0, True)
            pass_on(0, False)
            send(here, here, sd_s.at[0, 0], sd_r.at[0, 0], mate).start()
            return
        pass_on(d, True)
        pass_on(d, False)

    def travelled(up, d):
        j = f - d if up else f + d
        lane = 0 if up else 1

        @pl.when(jnp.logical_and(j >= 0, j < nfs))
        def _():
            spot = strip(1 - side, other, j)
            arrived(spot, sd_r.at[lane, d])
            left(spot, sd_s.at[lane, d])

    def sent_on(up, d):
        j = f - d if up else f + d
        ahead = f + 1 if up else f - 1
        lane = 0 if up else 1
        inside = jnp.logical_and(j >= 0, j < nfs)
        more = jnp.logical_and(ahead >= 0, ahead < nfs)
        pl.when(jnp.logical_and(inside, more))(
            lambda: left(strip(1 - side, r, j), st_s.at[lane, d])
        )

    for b in range(blocks):
        a, c = b // wide_b, b % wide_b
        start = other * (small // 2) + a * half
        arrived(gb.at[at(start, half, half), c * width : (c + 1) * width], gd_r.at[b])
    sums[...] = jnp.zeros_like(sums)
    for i in range(0, small, width):
        for j in range(0, small, width):
            if i == j:
                survey(gb, i, j, True, width)
            if i < j:
                survey(gb, i, j, False, width)
    inverse_b, scale_b = scales()

    def square(lhs, rhs, out, finish):
        def step(n, carry):
            i, j = n // (small // tile), n % (small // tile)
            rows, cols = at(i * tile, tile, tile), at(j * tile, tile, tile)
            acc = jnp.dot(lhs[rows, :small], rhs[:small, cols], preferred_element_type=F32)
            out[rows, cols] = finish(acc, lhs, rows, cols, (j - i) * tile).astype(BF16)
            return carry

        lax.fori_loop(0, (small // tile) ** 2, step, 0)

    square(gb, gb, b1, poly_one(inverse_b))
    square(gb, b1, b2, times(inverse_b))
    travel(0)
    square(b2, b1, b0, plain)
    square(b0, b0, b2, poly_two)
    travel(1)
    c2[:thin, :small] = b2[at(t * thin, thin, thin), :small]

    def tasks_b(n):
        if n == 3 and nfs > 2:
            travel(2)

    factor(
        thin, t * thin, 0, view(b0, 0, small), view(b1, 0, small), view(b2, 0, small),
        small, scale_b, put_qb, tasks_b,
    )

    def update(m, lhs, rhs, rate, ref, rows_of, step):
        def body(rows):
            acc = lax.dot_general(
                lhs(rows), rhs(), (((1,), (1,)), ((), ())), preferred_element_type=F32
            )
            ref(rows, acc, rate)

        rows_loop(rows_of, step, body)

    def put_big(m):
        def write(rows, acc, rate):
            vel[m, rows, :] = SHRINK * vel[m, rows, :] - rate * acc

        return write

    def put_small(rows, acc, rate):
        velb[rows, :] = SHRINK * velb[rows, :] - rate * acc

    rate = RATE * math.sqrt(height * nfs * 2)
    rate_b = RATE * math.sqrt(low * nfs * 2)

    def finish_big(m):
        update(m, lambda rows: s[m, rows, :], lambda: qt[m], rate, put_big(m), height, CHUNK)

        @pl.when(m == 0)
        def _():
            local(speed[0], gu, 15).start()

        @pl.when(m == 1)
        def _():
            local(speed[1], uu, 16).start()

    for m in range(3):
        local(weights[m], speed[m], 12 + m).wait()
    update(2, lambda rows: sb[rows, :], lambda: qtb[...], rate_b, put_small, low, CHUNK)
    local(velb, bu, 17).start()
    ring_in(0, ntp - 1)
    ring_in(1, 1)
    ring_in(1 - side, 2)
    arrived(qt.at[side, at(other * half, half, half)], q_r)
    finish_big(side)
    for d in range(3, nfs):
        travel(d)
    travelled(True, 0)
    for d in range(1, nfs):
        travelled(True, d)
        travelled(False, d)
    finish_big(1 - side)

    for m in range(3):
        for d in range(1, ntp):
            block = s.at[m, :, mine] if m < 2 else sb.at[:, mine_b]
            left(block, ring_s.at[m, d])
    for b in range(blocks):
        chain_end(b, 5 + b)
        left(tot.at[b], gd_s.at[b])
    left(qs, x_s)
    left(landing, q_s)
    for d in range(nfs - 1):
        sent_on(True, d)
        sent_on(False, d)
    local(speed[0], gu, 15).wait()
    local(speed[1], uu, 16).wait()
    local(velb, bu, 17).wait()


def hand_over(*refs):
    count = (len(refs) - 2) // 3
    sources, targets, stages = refs[:count], refs[count : 2 * count], refs[2 * count : 3 * count]
    came, went = refs[3 * count :]
    moves = []
    for i in range(count):
        rows = sources[i].shape[0]
        for j, top in enumerate((0, rows // 2)):
            span = pl.ds(top, rows // 2)
            stage = stages[i].at[span]
            moves.append(
                (
                    pltpu.make_async_copy(sources[i].at[span], stage, came.at[i, j]),
                    pltpu.make_async_copy(stage, targets[i].at[span], went.at[i, j]),
                )
            )
    for take, _ in moves:
        take.start()
    for take, give in moves:
        take.wait()
        give.start()
    for _, give in moves:
        give.wait()


def local_part(nfs, ntp, *args):
    height, width = args[1].shape
    low, thin = args[7].shape
    size, small = width * ntp, thin * ntp
    half = width // 2
    blocks = small // 2 // half * (small // width)
    vmem = pltpu.VMEM
    dma = pltpu.SemaphoreType.DMA
    scratch = [
        vmem((2, height, size), BF16),
        vmem((low, small), BF16),
        vmem((2, height, width), F32),
        vmem((low, thin), F32),
        vmem((2, height, width), F32),
        vmem((low, thin), F32),
        vmem((2, height, width), F32),
        vmem((low, thin), F32),
    ]
    scratch += [vmem((5, half, width), BF16)] * 4
    scratch += [vmem((5 + blocks, half, width), BF16), vmem((5, half, width), BF16)]
    scratch += [vmem((size, size), BF16)] * 3 + [vmem((small, small), BF16)]
    scratch += [vmem((half + half // nfs, size), BF16)] * 3 + [vmem((half // nfs, size), BF16)]
    scratch += [vmem((2, width, size), BF16), vmem((thin, small), BF16), vmem((2, 8, width), F32)]
    slots = dma((5 + blocks,))
    scratch += [dma((18,)), dma((3,)), dma((3,)), dma((3, ntp)), dma((3, ntp))]
    scratch += [slots] * 7
    scratch += [dma((5, 2)), dma((10,)), dma((10,)), dma((10,)), dma((blocks,)), dma((blocks,))]
    scratch += [dma((4, 5)), dma((4, 5))] + [dma] * 4 + [dma((2, nfs))] * 4
    outs = []
    for i in range(3):
        outs += [jax.ShapeDtypeStruct(args[3 * i + 1].shape, F32)] * 2
    results = pl.pallas_call(
        functools.partial(kernel, nfs, ntp),
        out_shape=tuple(outs),
        in_specs=[pl.BlockSpec(memory_space=pl.ANY)] * 9,
        out_specs=tuple([pl.BlockSpec(memory_space=pl.ANY)] * 6),
        scratch_shapes=scratch,
        compiler_params=pltpu.CompilerParams(
            collective_id=0, has_side_effects=True, vmem_limit_bytes=GRANT
        ),
        name="orthogonal",
    )(*args)
    dma2 = dma((len(outs), 2))
    return pl.pallas_call(
        hand_over,
        out_shape=tuple(outs),
        in_specs=[pl.BlockSpec(memory_space=pl.ANY)] * len(outs),
        out_specs=tuple([pl.BlockSpec(memory_space=pl.ANY)] * len(outs)),
        scratch_shapes=[vmem(o.shape, F32) for o in outs] + [dma2, dma2],
        name="hand_over",
    )(*results)


def solution(mesh):
    sizes = mesh.shape
    split = P(("fs", "rep"), "tp")
    return jax.shard_map(
        functools.partial(local_part, sizes["fs"], sizes["tp"]),
        mesh=mesh,
        in_specs=(P("rep", "fs", "tp"), split, split) * 3,
        out_specs=(split,) * 6,
        check_vma=False,
    )
```

```python
import functools
import math

import jax
import jax.numpy as jnp
from jax import lax
from jax.experimental import pallas as pl
from jax.experimental.pallas import tpu as pltpu
from jax.sharding import PartitionSpec as P

MOMENT = 0.95
COEF_ONE = 3.4445
COEF_THREE = -4.775
COEF_FIVE = 2.0315
SAFETY = 2.0
RATE = 0.5
SHRINK = 0.95
STEP = 64
CHUNK = 176
GRANT = 67043328
F32 = jnp.float32
BF16 = jnp.bfloat16


def at(start, size, unit):
    return pl.ds(pl.multiple_of(start, unit), size)


def fit(rows, most):
    return max(n for n in range(16, most + 1, 16) if rows % n == 0)


def rows_loop(rows, most, body):
    step = fit(rows, most)

    def run(i, carry):
        body(at(i * step, step, step))
        return carry

    lax.fori_loop(0, rows // step, run, 0)


def kernel(nfs, ntp, *refs):
    (gg, gv, gw, ug, uv, uw, bg, bv, bw, gm, gu, um, uu, bm, bu) = refs[:15]
    (s, sb, vel, velb, gs, gsb, go, gob) = refs[15:23]
    (psend, part, prcv, rin, cross, tot, b0, b1, b2, gb) = refs[23:33]
    (c0, c1, c2, qs, qt, qtb, sums) = refs[33:40]
    (loc, rep_s, rep_r, ring_s, ring_r, half_s, half_r, in_s, in_r, mid_r) = refs[40:50]
    (out_s, out_r, ag_s, ag_r, dd_s, dd_r, gd_s, gd_r, pr_s, pr_r, q_s, q_r) = refs[50:62]
    (x_s, x_r, st_s, st_r, sd_s, sd_r) = refs[62:68]

    height, size = s.shape[1:]
    width = size // ntp
    half = width // 2
    low, small = sb.shape
    thin = small // ntp
    count = 4
    tile = size // count

    f, t, r = lax.axis_index("fs"), lax.axis_index("tp"), lax.axis_index("rep")

    def turn(v):
        return v + v // 2 * (5 - 2 * v)

    p = turn(t)
    side = t % 2
    other = 1 - r
    peers = [turn((p + d) % ntp) for d in range(ntp)]
    across, beside, diagonal = t + 1 - 2 * side, (t + 2) % ntp, None
    diagonal = (across + 2) % ntp
    first_end, last_end = f == 0, f == nfs - 1
    is_end = jnp.logical_or(first_end, last_end)
    middle = nfs // 2
    is_mid = jnp.logical_or(f == middle - 1, f == middle)
    inward = jnp.where(f < middle, f + 1, f - 1)
    outward = jnp.where(f < middle, f - 1, f + 1)
    mate = {"rep": other}

    def send(src, dst, ssem, rsem, device):
        copy = pltpu.make_async_remote_copy(
            src_ref=src,
            dst_ref=dst,
            send_sem=ssem,
            recv_sem=rsem,
            device_id=device,
            device_id_type=pl.DeviceIdType.MESH,
        )
        return copy

    def arrived(dst, rsem):
        send(dst, dst, rsem, rsem, mate).wait_recv()

    def left(src, ssem):
        send(src, src, ssem, ssem, mate).wait_send()

    barrier = pltpu.get_barrier_semaphore()

    def greet(device):
        pl.semaphore_signal(
            barrier, inc=1, device_id=device, device_id_type=pl.DeviceIdType.MESH
        )

    grads, velocities, weights = (gg, ug, bg), (gv, uv, bv), (gw, uw, bw)
    outs_m, outs_u = (gm, um, bm), (gu, uu, bu)
    extents = ((height, width), (height, width), (low, thin))
    sent32 = (gs.at[0], gs.at[1], gsb)
    own32 = (go.at[0], go.at[1], gob)
    speed = (vel.at[0], vel.at[1], velb)
    txs = tuple(b1.at[:n, m * width : m * width + c] for m, (n, c) in enumerate(extents))
    rxs = tuple(b2.at[:n, m * width : m * width + c] for m, (n, c) in enumerate(extents))

    def local(src, dst, index):
        return pltpu.make_async_copy(src, dst, loc.at[index])

    loads = []
    for m in range(3):
        n = extents[m][0]
        loads.append(
            (
                local(grads[m].at[0, at(other * n, n, n)], sent32[m], m),
                local(grads[m].at[0, at(r * n, n, n)], own32[m], 3 + m),
                local(velocities[m], speed[m], 6 + m),
            )
        )
    for m in range(3):
        loads[m][0].start()
    for m in range(3):
        loads[m][1].start()
        loads[m][2].start()

    greet(mate)
    for d in range(1, ntp):
        greet({"tp": peers[d]})
    pl.when(f > 0)(lambda: greet({"fs": f - 1}))
    pl.when(f < nfs - 1)(lambda: greet({"fs": f + 1}))
    pl.semaphore_wait(barrier, ntp + jnp.minimum(f, 1) + jnp.minimum(nfs - 1 - f, 1))

    for m in range(3):
        loads[m][0].wait()

        def narrow(rows, m=m):
            txs[m][rows, :] = sent32[m][rows, :].astype(BF16)

        rows_loop(extents[m][0], STEP, narrow)
        send(txs[m], rxs[m], rep_s.at[m], rep_r.at[m], mate).start()

    mine = at(t * width, width, width)
    mine_b = at(t * thin, thin, thin)

    def ring(m, d):
        src = s.at[m, :, mine]
        send(src, src, ring_s.at[m, d], ring_r.at[m, d], {"tp": peers[d]}).start()

    def ring_b(d):
        src = sb.at[:, mine_b]
        send(src, src, ring_s.at[2, d], ring_r.at[2, d], {"tp": peers[d]}).start()

    def ring_in(m, d):
        spot = s.at[m, :, at(peers[ntp - d] * width, width, width)]
        arrived(spot, ring_r.at[m, d])

    def momentum(m):
        loads[m][1].wait()
        loads[m][2].wait()
        arrived(rxs[m], rep_r.at[m])

        def add(rows):
            total = own32[m][rows, :] + rxs[m][rows, :].astype(F32)
            value = MOMENT * speed[m][rows, :] + total
            speed[m][rows, :] = value
            if m < 2:
                s[m, rows, mine] = value.astype(BF16)
            else:
                sb[rows, mine_b] = value.astype(BF16)

        rows_loop(extents[m][0], STEP, add)
        local(speed[m], outs_m[m], 9 + m).start()

    def exchange(b, i, make):
        psend[b] = make(other)
        send(psend.at[b], prcv.at[b], half_s.at[i], half_r.at[i], mate).start()
        part[b] = make(r)

    def gram(slot, m, a, b):
        lo, hi = jnp.minimum(a, b), jnp.maximum(a, b)

        def make(h):
            return lax.dot_general(
                s[m, :, at(lo * width + h * half, half, half)],
                s[m, :, at(hi * width, width, width)],
                (((0,), (0,)), ((), ())),
                preferred_element_type=F32,
            ).astype(BF16)

        exchange(slot, slot, make)

    shares = {0: 1, 1: 2, 2: 4}

    def cut(c, n):
        return pl.ds(c * (half // n), half // n)

    def add_into(out, b, span, ref):
        def add(rows):
            rows = at(span.start + rows.start, rows.size, rows.size)
            value = part[b, rows, :].astype(F32) + ref[rows, :].astype(F32)
            out[b, rows, :] = value.astype(BF16)

        rows_loop(span.size, STEP, add)

    def to_inner(b, i, c, n):
        src, dst = part.at[b, cut(c, n)], rin.at[b, cut(c, n)]
        send(src, dst, in_s.at[i, c], in_r.at[i, c], {"fs": inward}).start()

    def to_outer(b, i, c, n):
        src = tot.at[b, cut(c, n)]
        send(src, src, out_s.at[i, c], out_r.at[i, c], {"fs": outward}).start()

    def chain_a(b, i, n=1):
        arrived(prcv.at[b], half_r.at[i])
        for c in range(n):
            add_into(part, b, cut(c, n), prcv.at[b])
            pl.when(jnp.logical_and(is_end, jnp.logical_not(is_mid)))(
                lambda c=c: to_inner(b, i, c, n)
            )

    def chain_b(b, i, c=0, n=1):
        span = cut(c, n)

        @pl.when(jnp.logical_not(is_end))
        def _():
            arrived(rin.at[b, span], in_r.at[i, c])
            add_into(part, b, span, rin.at[b])
            pl.when(jnp.logical_not(is_mid))(lambda: to_inner(b, i, c, n))

        @pl.when(is_mid)
        def _():
            src, dst = part.at[b, span], cross.at[i, span]
            send(src, dst, in_s.at[i, c], mid_r.at[i, c], {"fs": inward}).start()

    def chain_c(b, i, c=0, n=1, then=None):
        span = cut(c, n)

        @pl.when(is_mid)
        def _():
            arrived(cross.at[i, span], mid_r.at[i, c])
            add_into(tot, b, span, cross.at[i])
            pl.when(jnp.logical_not(is_end))(lambda: to_outer(b, i, c, n))
            if then is not None:
                then(b, c)

    def chain_d(b, i, c=0, n=1, then=None):
        @pl.when(jnp.logical_not(is_mid))
        def _():
            arrived(tot.at[b, cut(c, n)], out_r.at[i, c])
            pl.when(jnp.logical_not(is_end))(lambda: to_outer(b, i, c, n))
            if then is not None:
                then(b, c)

    def chain_end(b, i, n=1):
        left(psend.at[b], half_s.at[i])
        for c in range(n):
            left(part.at[b, cut(c, n)], in_s.at[i, c])
            pl.when(jnp.logical_not(is_end))(
                lambda c=c: left(tot.at[b, cut(c, n)], out_s.at[i, c])
            )

    def place(q, kind, matrix):
        a = turn(q)
        b = {
            0: a,
            1: turn((q + ntp - 1 + 2 * matrix) % ntp),
            2: turn((q + ntp // 2) % ntp),
        }[kind]
        return jnp.minimum(a, b), jnp.maximum(a, b)

    def spot(q, kind, matrix, h, c=0, n=1):
        i, j = place(q, kind, matrix)
        top = i * width + h * half + c * (half // n)
        return b0.at[at(top, half // n, half // n), at(j * width, width, width)]

    kinds = (0, 1, 2, 0, 1, 0, 1, 2, 0, 1)
    owners = [p] * 3 + [turn(across)] * 2 + [turn(beside)] * 3 + [turn(diagonal)] * 2

    def gather_own(slot, kind, matrix, c):
        n = shares[kind]
        here, src = spot(p, kind, matrix, r, c, n), tot.at[slot, cut(c, n)]
        i, j = place(p, kind, matrix)
        top = c * (half // n)

        def copy(rows):
            to = at(i * width + r * half + top + rows.start, rows.size, rows.size)
            b0[to, at(j * width, width, width)] = tot[
                slot, at(top + rows.start, rows.size, rows.size), :
            ]

        rows_loop(half // n, STEP, copy)
        send(
            src, here, ag_s.at[slot, c, 0], ag_r.at[5 + kind, c], {"tp": beside}
        ).start()
        send(src, here, dd_s.at[kind, c], dd_r.at[kind, c], mate).start()

    def gather_far(slot, kind, matrix, c):
        n = shares[kind]
        here, src = spot(p, kind, matrix, r, c, n), tot.at[slot, cut(c, n)]
        send(
            src, here, ag_s.at[slot, c, 0], ag_r.at[3 + kind, c], {"tp": across}
        ).start()
        send(
            src, here, ag_s.at[slot, c, 1], ag_r.at[8 + kind, c], {"tp": diagonal}
        ).start()

    def gather(slot, c):
        if slot == 4:
            gather_own(slot, 2, side, c)
            return
        matrix, kind = slot // 2, slot % 2
        pl.when(side == matrix)(lambda: gather_own(slot, kind, matrix, c))
        pl.when(side != matrix)(lambda: gather_far(slot, kind, matrix, c))

    momentum(0)
    ring(0, 1)
    momentum(1)
    ring(1, ntp - 1)
    ring(1 - side, 2)
    gram(0, 0, t, t)
    gram(2, 1, t, t)
    momentum(2)
    chain_a(0, 0)
    chain_a(2, 2)
    chain_b(0, 0)
    chain_b(2, 2)
    ring_in(0, 1)
    gram(1, 0, peers[ntp - 1], t)
    ring_in(1, ntp - 1)
    gram(3, 1, peers[1], t)
    few, many = shares[1], shares[2]
    chain_a(1, 1, few)
    chain_a(3, 3, few)
    chain_c(0, 0, then=gather)
    chain_c(2, 2, then=gather)
    for slot in (1, 3):
        for c in range(few):
            chain_b(slot, slot, c, few)
    chain_d(0, 0, then=gather)
    chain_d(2, 2, then=gather)
    ring_in(side, 2)
    gram(4, side, peers[2], t)
    chain_a(4, 4, many)
    for slot in (1, 3):
        for c in range(few):
            chain_c(slot, slot, c, few, gather)
    for c in range(many + 1):
        if c < many:
            chain_b(4, 4, c, many)
        if c > 0:
            chain_c(4, 4, c - 1, many, gather)
    for slot in (1, 3):
        for c in range(few):
            chain_d(slot, slot, c, few, gather)
    for c in range(many):
        chain_d(4, 4, c, many, gather)

    for m in range(3):
        left(txs[m], rep_s.at[m])

    def forward(e):
        n = shares[kinds[e]]
        for c in range(n):
            here = spot(owners[e], kinds[e], side, r, c, n)
            arrived(here, ag_r.at[e, c])
            send(here, here, dd_s.at[e, c], dd_r.at[e, c], mate).start()

    sums[...] = jnp.zeros_like(sums)

    def fold(value):
        return jnp.sum(value.reshape(-1, 8, value.shape[1]), axis=0)

    def survey(ref, i, j, diag, span):
        def add(rows):
            wide = ref[at(i + rows.start, STEP, STEP), at(j, span, span)].astype(F32)
            weight = 1.0 if diag else 2.0
            sums[1, :, :span] += weight * fold(wide * wide)
            if diag:
                down = lax.broadcasted_iota(jnp.int32, wide.shape, 0) + rows.start
                over = lax.broadcasted_iota(jnp.int32, wide.shape, 1)
                sums[0, :, :span] += fold(jnp.where(down == over, wide, 0.0))

        rows_loop(span, STEP, add)

    def scales():
        first = jnp.sum(jnp.sum(sums[0], axis=0, keepdims=True), axis=1, keepdims=True)
        second = jnp.sum(jnp.sum(sums[1], axis=0, keepdims=True), axis=1, keepdims=True)
        ratio = SAFETY * (second + 1.0) / (first + 1.0)
        return 1.0 / ratio, lax.rsqrt(ratio)

    def digest(e):
        n = shares[kinds[e]]
        for c in range(n):
            arrived(spot(owners[e], kinds[e], side, other, c, n), dd_r.at[e, c])
        i, j = place(owners[e], kinds[e], side)
        survey(b0, i * width, j * width, kinds[e] == 0, width)
        if kinds[e] != 0:
            b0[at(j * width, width, width), at(i * width, width, width)] = b0[
                at(i * width, width, width), at(j * width, width, width)
            ].T

    for e in (3, 5, 8):
        forward(e)
    for e in (0, 3, 5, 8):
        digest(e)
    for e in (4, 6, 9):
        forward(e)
    for e in (1, 4, 6, 9):
        digest(e)
    forward(7)
    digest(2)
    digest(7)

    for slot in range(5):
        n = shares[2] if slot == 4 else shares[slot % 2]
        chain_end(slot, slot, n)
        for c in range(n):
            piece = tot.at[slot, cut(c, n)]
            left(piece, ag_s.at[slot, c, 0])
            if slot < 4:
                pl.when(side != slot // 2)(
                    lambda piece=piece, slot=slot, c=c: left(piece, ag_s.at[slot, c, 1])
                )
    for e in range(10):
        n = shares[kinds[e]]
        for c in range(n):
            left(tot.at[0, cut(0, n)], dd_s.at[e, c])
    for d in range(1, ntp):
        ring_b(d)
    ring(0, ntp - 1)
    ring(1, 1)
    ring(side, 2)
    for m in range(3):
        local(speed[m], outs_m[m], 9 + m).wait()
        local(weights[m], speed[m], 12 + m).start()

    inverse, scale = scales()

    def eye(shape, shift):
        down = lax.broadcasted_iota(jnp.int32, shape, 0)
        over = lax.broadcasted_iota(jnp.int32, shape, 1)
        return jnp.where(down == over + shift, COEF_ONE, 0.0)

    def product(index, span, lhs, rhs, out, finish, before, after=None):
        step = span // count

        def where(k, who):
            i, j = k // 4, jnp.where(k == 1, 3, jnp.where(k > 1, k - 1 - k // 4 * 2, 0))
            odd = jnp.where(k == 1, 1, 0)
            i, j = i + who * (3 - j + odd - i), j + who * (3 - i - odd - j)
            return i, j, at(i * step, step, step), at(j * step, step, step)

        def compute(k):
            i, j, rows, cols = where(k, r)
            acc = jnp.dot(lhs[rows, :span], rhs[:span, cols], preferred_element_type=F32)
            value = finish(acc, lhs, rows, cols, (j - i) * step).astype(BF16)
            out[rows, cols] = value

            @pl.when(i != j)
            def _():
                out[cols, rows] = value.T

        def ship(k):
            _, _, rows, cols = where(k, r)
            here = out.at[rows, cols]
            send(here, here, pr_s.at[index, k], pr_r.at[index, k], mate).start()

        def take(k):
            i, j, rows, cols = where(k, other)
            here = out.at[rows, cols]
            arrived(here, pr_r.at[index, k])

            @pl.when(i != j)
            def _():
                out[cols, rows] = out[rows, cols].T

            left(here, pr_s.at[index, k])

        compute(0)
        before()
        ship(0)

        def run(k, carry):
            compute(k)
            ship(k)
            return carry

        lax.fori_loop(1, 5, run, 0)
        if after is not None:
            after()
        take(1)

        def rest(n, carry):
            take(n + jnp.minimum(n, 1))
            return carry

        return lambda: lax.fori_loop(0, 4, rest, 0)

    def poly_one(inv):
        def finish(acc, lhs, rows, cols, shift):
            gram_part = lhs[rows, cols].astype(F32) * inv
            return eye(acc.shape, shift) + COEF_THREE * gram_part + COEF_FIVE * (acc * inv * inv)

        return finish

    def times(inv):
        return lambda acc, lhs, rows, cols, shift: acc * inv

    def plain(acc, lhs, rows, cols, shift):
        return acc

    def poly_two(acc, lhs, rows, cols, shift):
        return eye(acc.shape, shift) + COEF_THREE * lhs[rows, cols].astype(F32) + COEF_FIVE * acc

    done = product(0, size, b0, b0, b1, poly_one(inverse), lambda: None)

    blocks = 3

    def block(b, who):
        i, j = (2 * who + b, who) if b < 2 else (who, 1)
        return i * half, j * width

    def branch_gram():
        for d in range(1, ntp):
            arrived(sb.at[:, at(peers[ntp - d] * thin, thin, thin)], ring_r.at[2, d])
        for b in range(blocks):
            def make(who, b=b):
                i, j = block(b, who)
                return lax.dot_general(
                    sb[:, at(i, half, half)],
                    sb[:, at(j, width, width)],
                    (((0,), (0,)), ((), ())),
                    preferred_element_type=F32,
                ).astype(BF16)

            exchange(b, 5 + b, make)

    def settle(b):
        chain_d(b, 5 + b)
        i, j = block(b, r)

        def copy(rows):
            gb[at(i + rows.start, STEP, STEP), at(j, width, width)] = tot[b, rows, :]

        rows_loop(half, STEP, copy)
        here = gb.at[at(i, half, half), at(j, width, width)]
        send(tot.at[b], here, gd_s.at[b], gd_r.at[b], mate).start()

    done = product(1, size, b0, b1, b2, times(inverse), done, branch_gram)

    def begin_chain(first):
        first()
        for b in range(blocks):
            chain_a(b, 5 + b)

    done = product(2, size, b2, b1, b0, plain, functools.partial(begin_chain, done))
    chain_b(0, 5)
    done = product(3, size, b0, b0, b2, poly_two, done)
    chain_b(1, 6)
    chain_c(0, 5)
    done()

    def panel(lhs, rhs, out, span, finish):
        def step(j, carry):
            cols = at(j * tile, tile, tile)
            acc = jnp.dot(lhs(), rhs(cols), preferred_element_type=F32)
            out(cols, finish(acc, cols).astype(BF16))
            return carry

        lax.fori_loop(0, span // tile, step, 0)

    def same(acc, cols):
        return acc

    def factor(rows, begin, extra, g2, p1, p2, span, scaling, out, tasks):
        def buf(ref):
            return lambda: ref[:rows, :span]

        def put(ref):
            def write(cols, value):
                ref[:rows, cols] = value

            return write

        def cubic(acc, cols):
            down = lax.broadcasted_iota(jnp.int32, acc.shape, 0)
            over = lax.broadcasted_iota(jnp.int32, acc.shape, 1)
            down = down + jnp.where(down < half, begin, extra - half)
            unit = jnp.where(down == over + cols.start, COEF_ONE, 0.0)
            return unit + COEF_THREE * c1[:rows, cols].astype(F32) + COEF_FIVE * acc

        panel(buf(c2), p2, put(c0), span, same)
        tasks(0)
        panel(buf(c0), g2, put(c1), span, same)
        tasks(1)
        panel(buf(c1), g2, put(c2), span, same)
        tasks(2)
        panel(buf(c2), p2, put(c0), span, same)
        tasks(3)
        panel(buf(c0), p2, put(c2), span, cubic)
        tasks(4)
        panel(buf(c2), p2, put(c0), span, same)
        tasks(5)
        panel(buf(c0), p1, out, span, lambda acc, cols: acc * scaling)

    def view(ref, top, span):
        return lambda cols: ref[top : top + span, cols]

    slab = half // nfs
    begin, extra = t * width + r * half, across * width + r * half + f * slab

    def put_q(cols, value):
        qt[side, at(r * half, half, half), cols] = value[:half]
        qs[:, cols] = value[half:]

    def put_qb(cols, value):
        qtb[:, cols] = value

    def fill(rows):
        c2[rows, :] = b2[at(begin + rows.start, STEP, STEP), :]

    rows_loop(half, STEP, fill)
    c2[half : half + slab, :] = b2[at(extra, slab, slab), :]

    def tasks(n):
        if n == 0:
            chain_b(2, 7)
        if n == 1:
            chain_c(1, 6)
        if n == 2:
            chain_c(2, 7)
        if n == 3:
            settle(0)
        if n == 5:
            settle(1)
            settle(2)

    factor(
        half + slab, begin, extra, view(b0, 0, size), view(b1, 0, size), view(b2, 0, size),
        size, scale, put_q, tasks,
    )

    chunk = size // 2

    def strip(m, who, j, c):
        return qt.at[m, at(who * half + j * slab, slab, slab), c * chunk : (c + 1) * chunk]

    for c in range(2):
        piece = qs.at[:, c * chunk : (c + 1) * chunk]
        send(piece, strip(side, r, f, c), x_s.at[c], x_r.at[c], {"tp": across}).start()
    landing = qt.at[side, at(r * half, half, half)]
    send(landing, landing, q_s, q_r, mate).start()

    def course(d, up):
        j, ahead = (f - d, f + 1) if up else (f + d, f - 1)
        inside = jnp.logical_and(j >= 0, j < nfs)
        more = jnp.logical_and(ahead >= 0, ahead < nfs)
        return 0 if up else 1, j, ahead, inside, more

    def pass_on(d, c, up):
        lane, j, ahead, inside, more = course(d, up)

        def onward(spot):
            send(
                spot, spot, st_s.at[lane, 2 * d + c], st_r.at[lane, 2 * d + 2 + c], {"fs": ahead}
            ).start()

        if d == 0:
            pl.when(more)(lambda: onward(strip(1 - side, r, f, c)))
            return

        @pl.when(inside)
        def _():
            spot = strip(1 - side, r, j, c)
            arrived(spot, st_r.at[lane, 2 * d + c])
            pl.when(more)(lambda: onward(spot))
            send(
                spot, spot, sd_s.at[lane, 2 * d + c], sd_r.at[lane, 2 * d + c], mate
            ).start()

    def travel(d, c):
        if d >= nfs:
            return
        if d == 0:
            arrived(strip(1 - side, r, f, c), x_r.at[c])
        pass_on(d, c, True)
        pass_on(d, c, False)
        if d == 0:
            here = strip(1 - side, r, f, c)
            send(here, here, sd_s.at[0, c], sd_r.at[0, c], mate).start()

    def travelled(d, c, up):
        lane, j, ahead, inside, more = course(d, up)

        @pl.when(inside)
        def _():
            spot = strip(1 - side, other, j, c)
            arrived(spot, sd_r.at[lane, 2 * d + c])
            left(spot, sd_s.at[lane, 2 * d + c])

    def sent_on(d, c, up):
        lane, j, ahead, inside, more = course(d, up)
        pl.when(jnp.logical_and(inside, more))(
            lambda: left(strip(1 - side, r, j, c), st_s.at[lane, 2 * d + c])
        )

    for b in range(blocks):
        i, j = block(b, other)
        arrived(gb.at[at(i, half, half), at(j, width, width)], gd_r.at[b])
    sums[...] = jnp.zeros_like(sums)
    survey(gb, 0, 0, True, width)
    survey(gb, width, width, True, width)
    survey(gb, 0, width, False, width)
    gb[width:, :width] = gb[:width, width:].T
    inverse_b, scale_b = scales()
    both = lambda: arrived(qt.at[side, at(other * half, half, half)], q_r)
    done = product(4, small, gb, gb, b1, poly_one(inverse_b), both)
    done = product(5, small, gb, b1, b2, times(inverse_b), done)
    travel(0, 0)
    done = product(6, small, b2, b1, b0, plain, done)
    travel(0, 1)
    done = product(7, small, b0, b0, b2, poly_two, done)
    travel(1, 0)
    done()
    c2[:thin, :small] = b2[at(t * thin, thin, thin), :small]

    def tasks_b(n):
        if n == 1:
            travel(1, 1)
        if n == 3:
            travel(2, 0)

    factor(
        thin, t * thin, 0, view(b0, 0, small), view(b1, 0, small), view(b2, 0, small),
        small, scale_b, put_qb, tasks_b,
    )

    def update(m, lhs, rhs, rate, ref, rows_of, step):
        def body(rows):
            acc = lax.dot_general(
                lhs(rows), rhs(), (((1,), (1,)), ((), ())), preferred_element_type=F32
            )
            ref(rows, acc, rate)

        rows_loop(rows_of, step, body)

    def put_big(m):
        def write(rows, acc, rate):
            vel[m, rows, :] = SHRINK * vel[m, rows, :] - rate * acc

        return write

    def put_small(rows, acc, rate):
        velb[rows, :] = SHRINK * velb[rows, :] - rate * acc

    rate = RATE * math.sqrt(height * nfs * 2)
    rate_b = RATE * math.sqrt(low * nfs * 2)

    def finish_big(m):
        update(m, lambda rows: s[m, rows, :], lambda: qt[m], rate, put_big(m), height, CHUNK)

        @pl.when(m == 0)
        def _():
            local(speed[0], gu, 15).start()

        @pl.when(m == 1)
        def _():
            local(speed[1], uu, 16).start()

    for m in range(3):
        local(weights[m], speed[m], 12 + m).wait()
    update(2, lambda rows: sb[rows, :], lambda: qtb[...], rate_b, put_small, low, CHUNK)
    local(velb, bu, 17).start()
    travel(2, 1)
    ring_in(0, ntp - 1)
    ring_in(1, 1)
    ring_in(1 - side, 2)
    finish_big(side)
    for d in range(3, nfs):
        travel(d, 0)
        travel(d, 1)
    for d in range(nfs):
        for c in range(2):
            travelled(d, c, True)
            if d > 0:
                travelled(d, c, False)
    finish_big(1 - side)

    for m in range(3):
        for d in range(1, ntp):
            block = s.at[m, :, mine] if m < 2 else sb.at[:, mine_b]
            left(block, ring_s.at[m, d])
    for b in range(blocks):
        chain_end(b, 5 + b)
        left(tot.at[b], gd_s.at[b])
    left(landing, q_s)
    for c in range(2):
        left(qs.at[:, c * chunk : (c + 1) * chunk], x_s.at[c])
        for d in range(nfs - 1):
            sent_on(d, c, True)
            sent_on(d, c, False)
    local(speed[0], gu, 15).wait()
    local(speed[1], uu, 16).wait()
    local(velb, bu, 17).wait()


def hand_over(*refs):
    count = (len(refs) - 2) // 3
    sources, targets, stages = refs[:count], refs[count : 2 * count], refs[2 * count : 3 * count]
    came, went = refs[3 * count :]
    moves = []
    for i in range(count):
        rows = sources[i].shape[0]
        for j, top in enumerate((0, rows // 2)):
            span = pl.ds(top, rows // 2)
            stage = stages[i].at[span]
            moves.append(
                (
                    pltpu.make_async_copy(sources[i].at[span], stage, came.at[i, j]),
                    pltpu.make_async_copy(stage, targets[i].at[span], went.at[i, j]),
                )
            )
    for take, _ in moves:
        take.start()
    for take, give in moves:
        take.wait()
        give.start()
    for _, give in moves:
        give.wait()


def local_part(nfs, ntp, *args):
    height, width = args[1].shape
    low, thin = args[7].shape
    size, small = width * ntp, thin * ntp
    half = width // 2
    blocks = 3
    vmem = pltpu.VMEM
    dma = pltpu.SemaphoreType.DMA
    scratch = [
        vmem((2, height, size), BF16),
        vmem((low, small), BF16),
        vmem((2, height, width), F32),
        vmem((low, thin), F32),
        vmem((2, height, width), F32),
        vmem((low, thin), F32),
        vmem((2, height, width), F32),
        vmem((low, thin), F32),
    ]
    scratch += [vmem((5, half, width), BF16)] * 4
    scratch += [vmem((5 + blocks, half, width), BF16), vmem((5, half, width), BF16)]
    scratch += [vmem((size, size), BF16)] * 3 + [vmem((small, small), BF16)]
    scratch += [vmem((half + half // nfs, size), BF16)] * 3 + [vmem((half // nfs, size), BF16)]
    scratch += [vmem((2, width, size), BF16), vmem((thin, small), BF16), vmem((2, 8, width), F32)]
    slots = dma((5 + blocks,))
    scratch += [dma((18,)), dma((3,)), dma((3,)), dma((3, ntp)), dma((3, ntp))]
    scratch += [slots] * 2 + [dma((5 + blocks, 4))] * 5
    scratch += [dma((5, 4, 2)), dma((10, 4)), dma((10, 4)), dma((10, 4)), dma((blocks,)), dma((blocks,))]
    scratch += [dma((8, 5))] * 2 + [dma, dma, dma((2,)), dma((2,))] + [dma((2, 2 * nfs))] * 4
    outs = []
    for i in range(3):
        outs += [jax.ShapeDtypeStruct(args[3 * i + 1].shape, F32)] * 2
    results = pl.pallas_call(
        functools.partial(kernel, nfs, ntp),
        out_shape=tuple(outs),
        in_specs=[pl.BlockSpec(memory_space=pl.ANY)] * 9,
        out_specs=tuple([pl.BlockSpec(memory_space=pl.ANY)] * 6),
        scratch_shapes=scratch,
        compiler_params=pltpu.CompilerParams(
            collective_id=0, has_side_effects=True, vmem_limit_bytes=GRANT
        ),
        name="orthogonal",
    )(*args)
    dma2 = dma((len(outs), 2))
    return pl.pallas_call(
        hand_over,
        out_shape=tuple(outs),
        in_specs=[pl.BlockSpec(memory_space=pl.ANY)] * len(outs),
        out_specs=tuple([pl.BlockSpec(memory_space=pl.ANY)] * len(outs)),
        scratch_shapes=[vmem(o.shape, F32) for o in outs] + [dma2, dma2],
        name="hand_over",
    )(*results)


def solution(mesh):
    sizes = mesh.shape
    split = P(("fs", "rep"), "tp")
    return jax.shard_map(
        functools.partial(local_part, sizes["fs"], sizes["tp"]),
        mesh=mesh,
        in_specs=(P("rep", "fs", "tp"), split, split) * 3,
        out_specs=(split,) * 6,
        check_vma=False,
    )
```

```python
import functools
import math

import jax
import jax.numpy as jnp
from jax import lax
from jax.experimental import pallas as pl
from jax.experimental.pallas import tpu as pltpu
from jax.sharding import PartitionSpec as P

MOMENT = 0.95
COEF_ONE = 3.4445
COEF_THREE = -4.775
COEF_FIVE = 2.0315
SAFETY = 2.0
RATE = 0.5
SHRINK = 0.95
STEP = 64
CHUNK = 176
GRANT = 67043328
F32 = jnp.float32
BF16 = jnp.bfloat16


def at(start, size, unit):
    return pl.ds(pl.multiple_of(start, unit), size)


def fit(rows, most):
    return max(n for n in range(16, most + 1, 16) if rows % n == 0)


def rows_loop(rows, most, body):
    step = fit(rows, most)

    def run(i, carry):
        body(at(i * step, step, step))
        return carry

    lax.fori_loop(0, rows // step, run, 0)


def kernel(nfs, ntp, *refs):
    (gg, gv, gw, ug, uv, uw, bg, bv, bw, gm, gu, um, uu, bm, bu) = refs[:15]
    (s, sb, vel, velb, gs, gsb, go, gob) = refs[15:23]
    (psend, part, prcv, rin, cross, tot, b0, b1, b2, gb) = refs[23:33]
    (c0, c1, c2, qs, qt, qtb, sums) = refs[33:40]
    (loc, rep_s, rep_r, ring_s, ring_r, half_s, half_r, in_s, in_r, mid_r) = refs[40:50]
    (out_s, out_r, ag_s, ag_r, dd_s, dd_r, gd_s, gd_r, pr_s, pr_r, q_s, q_r) = refs[50:62]
    (x_s, x_r, st_s, st_r, sd_s, sd_r) = refs[62:68]

    height, size = s.shape[1:]
    width = size // ntp
    half = width // 2
    low, small = sb.shape
    thin = small // ntp
    count = 4
    tile = size // count

    f, t, r = lax.axis_index("fs"), lax.axis_index("tp"), lax.axis_index("rep")

    def turn(v):
        return v + v // 2 * (5 - 2 * v)

    p = turn(t)
    side = t % 2
    other = 1 - r
    peers = [turn((p + d) % ntp) for d in range(ntp)]
    across, beside, diagonal = t + 1 - 2 * side, (t + 2) % ntp, None
    diagonal = (across + 2) % ntp
    first_end, last_end = f == 0, f == nfs - 1
    is_end = jnp.logical_or(first_end, last_end)
    middle = nfs // 2
    is_mid = jnp.logical_or(f == middle - 1, f == middle)
    inward = jnp.where(f < middle, f + 1, f - 1)
    outward = jnp.where(f < middle, f - 1, f + 1)
    mate = {"rep": other}

    def send(src, dst, ssem, rsem, device):
        copy = pltpu.make_async_remote_copy(
            src_ref=src,
            dst_ref=dst,
            send_sem=ssem,
            recv_sem=rsem,
            device_id=device,
            device_id_type=pl.DeviceIdType.MESH,
        )
        return copy

    def arrived(dst, rsem):
        send(dst, dst, rsem, rsem, mate).wait_recv()

    def left(src, ssem):
        send(src, src, ssem, ssem, mate).wait_send()

    barrier = pltpu.get_barrier_semaphore()

    def greet(device):
        pl.semaphore_signal(
            barrier, inc=1, device_id=device, device_id_type=pl.DeviceIdType.MESH
        )

    grads, velocities, weights = (gg, ug, bg), (gv, uv, bv), (gw, uw, bw)
    outs_m, outs_u = (gm, um, bm), (gu, uu, bu)
    extents = ((height, width), (height, width), (low, thin))
    sent32 = (gs.at[0], gs.at[1], gsb)
    own32 = (go.at[0], go.at[1], gob)
    speed = (vel.at[0], vel.at[1], velb)
    txs = tuple(b1.at[:n, m * width : m * width + c] for m, (n, c) in enumerate(extents))
    rxs = tuple(b2.at[:n, m * width : m * width + c] for m, (n, c) in enumerate(extents))

    def local(src, dst, index):
        return pltpu.make_async_copy(src, dst, loc.at[index])

    loads = []
    for m in range(3):
        n = extents[m][0]
        loads.append(
            (
                local(grads[m].at[0, at(other * n, n, n)], sent32[m], m),
                local(grads[m].at[0, at(r * n, n, n)], own32[m], 3 + m),
                local(velocities[m], speed[m], 6 + m),
            )
        )
    for m in range(3):
        loads[m][0].start()
    for m in range(3):
        loads[m][1].start()
        loads[m][2].start()

    greet(mate)
    for d in range(1, ntp):
        greet({"tp": peers[d]})
    pl.when(f > 0)(lambda: greet({"fs": f - 1}))
    pl.when(f < nfs - 1)(lambda: greet({"fs": f + 1}))
    pl.semaphore_wait(barrier, ntp + jnp.minimum(f, 1) + jnp.minimum(nfs - 1 - f, 1))

    for m in range(3):
        loads[m][0].wait()

        def narrow(rows, m=m):
            txs[m][rows, :] = sent32[m][rows, :].astype(BF16)

        rows_loop(extents[m][0], STEP, narrow)
        send(txs[m], rxs[m], rep_s.at[m], rep_r.at[m], mate).start()

    mine = at(t * width, width, width)
    mine_b = at(t * thin, thin, thin)

    def ring(m, d):
        src = s.at[m, :, mine]
        send(src, src, ring_s.at[m, d], ring_r.at[m, d], {"tp": peers[d]}).start()

    def ring_b(d):
        src = sb.at[:, mine_b]
        send(src, src, ring_s.at[2, d], ring_r.at[2, d], {"tp": peers[d]}).start()

    def ring_in(m, d):
        spot = s.at[m, :, at(peers[ntp - d] * width, width, width)]
        arrived(spot, ring_r.at[m, d])

    def momentum(m):
        loads[m][1].wait()
        loads[m][2].wait()
        arrived(rxs[m], rep_r.at[m])

        def add(rows):
            total = own32[m][rows, :] + rxs[m][rows, :].astype(F32)
            value = MOMENT * speed[m][rows, :] + total
            speed[m][rows, :] = value
            if m < 2:
                s[m, rows, mine] = value.astype(BF16)
            else:
                sb[rows, mine_b] = value.astype(BF16)

        rows_loop(extents[m][0], STEP, add)
        local(speed[m], outs_m[m], 9 + m).start()

    def exchange(b, i, make):
        psend[b] = make(other)
        send(psend.at[b], prcv.at[b], half_s.at[i], half_r.at[i], mate).start()
        part[b] = make(r)

    def gram(slot, m, a, b):
        lo, hi = jnp.minimum(a, b), jnp.maximum(a, b)

        def make(h):
            return lax.dot_general(
                s[m, :, at(lo * width + h * half, half, half)],
                s[m, :, at(hi * width, width, width)],
                (((0,), (0,)), ((), ())),
                preferred_element_type=F32,
            ).astype(BF16)

        exchange(slot, slot, make)

    shares = {0: 1, 1: 2, 2: 4}

    def cut(c, n):
        return pl.ds(c * (half // n), half // n)

    def add_into(out, b, span, ref):
        def add(rows):
            rows = at(span.start + rows.start, rows.size, rows.size)
            value = part[b, rows, :].astype(F32) + ref[rows, :].astype(F32)
            out[b, rows, :] = value.astype(BF16)

        rows_loop(span.size, STEP, add)

    def to_inner(b, i, c, n):
        src, dst = part.at[b, cut(c, n)], rin.at[b, cut(c, n)]
        send(src, dst, in_s.at[i, c], in_r.at[i, c], {"fs": inward}).start()

    def to_outer(b, i, c, n):
        src = tot.at[b, cut(c, n)]
        send(src, src, out_s.at[i, c], out_r.at[i, c], {"fs": outward}).start()

    def chain_a(b, i, n=1):
        arrived(prcv.at[b], half_r.at[i])
        for c in range(n):
            add_into(part, b, cut(c, n), prcv.at[b])
            pl.when(jnp.logical_and(is_end, jnp.logical_not(is_mid)))(
                lambda c=c: to_inner(b, i, c, n)
            )

    def chain_b(b, i, c=0, n=1):
        span = cut(c, n)

        @pl.when(jnp.logical_not(is_end))
        def _():
            arrived(rin.at[b, span], in_r.at[i, c])
            add_into(part, b, span, rin.at[b])
            pl.when(jnp.logical_not(is_mid))(lambda: to_inner(b, i, c, n))

        @pl.when(is_mid)
        def _():
            src, dst = part.at[b, span], cross.at[i, span]
            send(src, dst, in_s.at[i, c], mid_r.at[i, c], {"fs": inward}).start()

    def chain_c(b, i, c=0, n=1, then=None):
        span = cut(c, n)

        @pl.when(is_mid)
        def _():
            arrived(cross.at[i, span], mid_r.at[i, c])
            add_into(tot, b, span, cross.at[i])
            pl.when(jnp.logical_not(is_end))(lambda: to_outer(b, i, c, n))
            if then is not None:
                then(b, c)

    def chain_d(b, i, c=0, n=1, then=None):
        @pl.when(jnp.logical_not(is_mid))
        def _():
            arrived(tot.at[b, cut(c, n)], out_r.at[i, c])
            pl.when(jnp.logical_not(is_end))(lambda: to_outer(b, i, c, n))
            if then is not None:
                then(b, c)

    def chain_end(b, i, n=1):
        left(psend.at[b], half_s.at[i])
        for c in range(n):
            left(part.at[b, cut(c, n)], in_s.at[i, c])
            pl.when(jnp.logical_not(is_end))(
                lambda c=c: left(tot.at[b, cut(c, n)], out_s.at[i, c])
            )

    def place(q, kind, matrix):
        a = turn(q)
        b = {
            0: a,
            1: turn((q + ntp - 1 + 2 * matrix) % ntp),
            2: turn((q + ntp // 2) % ntp),
        }[kind]
        return jnp.minimum(a, b), jnp.maximum(a, b)

    def spot(q, kind, matrix, h, c=0, n=1):
        i, j = place(q, kind, matrix)
        top = i * width + h * half + c * (half // n)
        return b0.at[at(top, half // n, half // n), at(j * width, width, width)]

    kinds = (0, 1, 2, 0, 1, 0, 1, 2, 0, 1)
    owners = [p] * 3 + [turn(across)] * 2 + [turn(beside)] * 3 + [turn(diagonal)] * 2

    def gather_own(slot, kind, matrix, c):
        n = shares[kind]
        here, src = spot(p, kind, matrix, r, c, n), tot.at[slot, cut(c, n)]
        i, j = place(p, kind, matrix)
        top = c * (half // n)

        def copy(rows):
            to = at(i * width + r * half + top + rows.start, rows.size, rows.size)
            b0[to, at(j * width, width, width)] = tot[
                slot, at(top + rows.start, rows.size, rows.size), :
            ]

        rows_loop(half // n, STEP, copy)
        send(
            src, here, ag_s.at[slot, c, 0], ag_r.at[5 + kind, c], {"tp": beside}
        ).start()
        send(src, here, dd_s.at[kind, c], dd_r.at[kind, c], mate).start()

    def gather_far(slot, kind, matrix, c):
        n = shares[kind]
        here, src = spot(p, kind, matrix, r, c, n), tot.at[slot, cut(c, n)]
        send(
            src, here, ag_s.at[slot, c, 0], ag_r.at[3 + kind, c], {"tp": across}
        ).start()
        send(
            src, here, ag_s.at[slot, c, 1], ag_r.at[8 + kind, c], {"tp": diagonal}
        ).start()

    def gather(slot, c):
        if slot == 4:
            gather_own(slot, 2, side, c)
            return
        matrix, kind = slot // 2, slot % 2
        pl.when(side == matrix)(lambda: gather_own(slot, kind, matrix, c))
        pl.when(side != matrix)(lambda: gather_far(slot, kind, matrix, c))

    momentum(0)
    ring(0, 1)
    momentum(1)
    ring(1, ntp - 1)
    ring(1 - side, 2)
    gram(0, 0, t, t)
    gram(2, 1, t, t)
    momentum(2)
    chain_a(0, 0)
    chain_a(2, 2)
    chain_b(0, 0)
    chain_b(2, 2)
    ring_in(0, 1)
    gram(1, 0, peers[ntp - 1], t)
    ring_in(1, ntp - 1)
    gram(3, 1, peers[1], t)
    few, many = shares[1], shares[2]
    chain_a(1, 1, few)
    chain_a(3, 3, few)
    chain_c(0, 0, then=gather)
    chain_c(2, 2, then=gather)
    for slot in (1, 3):
        for c in range(few):
            chain_b(slot, slot, c, few)
    chain_d(0, 0, then=gather)
    chain_d(2, 2, then=gather)
    ring_in(side, 2)
    gram(4, side, peers[2], t)
    chain_a(4, 4, many)
    for slot in (1, 3):
        for c in range(few):
            chain_c(slot, slot, c, few, gather)
    for c in range(many + 1):
        if c < many:
            chain_b(4, 4, c, many)
        if c > 0:
            chain_c(4, 4, c - 1, many, gather)
    for slot in (1, 3):
        for c in range(few):
            chain_d(slot, slot, c, few, gather)
    for c in range(many):
        chain_d(4, 4, c, many, gather)

    for m in range(3):
        left(txs[m], rep_s.at[m])

    def forward(e):
        n = shares[kinds[e]]
        for c in range(n):
            here = spot(owners[e], kinds[e], side, r, c, n)
            arrived(here, ag_r.at[e, c])
            send(here, here, dd_s.at[e, c], dd_r.at[e, c], mate).start()

    sums[...] = jnp.zeros_like(sums)

    def fold(value):
        return jnp.sum(value.reshape(-1, 8, value.shape[1]), axis=0)

    def survey(ref, i, j, diag, span):
        def add(rows):
            wide = ref[at(i + rows.start, STEP, STEP), at(j, span, span)].astype(F32)
            weight = 1.0 if diag else 2.0
            sums[1, :, :span] += weight * fold(wide * wide)
            if diag:
                down = lax.broadcasted_iota(jnp.int32, wide.shape, 0) + rows.start
                over = lax.broadcasted_iota(jnp.int32, wide.shape, 1)
                sums[0, :, :span] += fold(jnp.where(down == over, wide, 0.0))

        rows_loop(span, STEP, add)

    def scales():
        first = jnp.sum(jnp.sum(sums[0], axis=0, keepdims=True), axis=1, keepdims=True)
        second = jnp.sum(jnp.sum(sums[1], axis=0, keepdims=True), axis=1, keepdims=True)
        ratio = SAFETY * (second + 1.0) / (first + 1.0)
        return 1.0 / ratio, lax.rsqrt(ratio)

    def digest(e):
        n = shares[kinds[e]]
        for c in range(n):
            arrived(spot(owners[e], kinds[e], side, other, c, n), dd_r.at[e, c])
        i, j = place(owners[e], kinds[e], side)
        survey(b0, i * width, j * width, kinds[e] == 0, width)
        if kinds[e] != 0:
            b0[at(j * width, width, width), at(i * width, width, width)] = b0[
                at(i * width, width, width), at(j * width, width, width)
            ].T

    for e in (3, 5, 8):
        forward(e)
    for e in (0, 3, 5, 8):
        digest(e)
    for e in (4, 6, 9):
        forward(e)
    for e in (1, 4, 6, 9):
        digest(e)
    forward(7)
    digest(2)
    digest(7)

    for slot in range(5):
        n = shares[2] if slot == 4 else shares[slot % 2]
        chain_end(slot, slot, n)
        for c in range(n):
            piece = tot.at[slot, cut(c, n)]
            left(piece, ag_s.at[slot, c, 0])
            if slot < 4:
                pl.when(side != slot // 2)(
                    lambda piece=piece, slot=slot, c=c: left(piece, ag_s.at[slot, c, 1])
                )
    for e in range(10):
        n = shares[kinds[e]]
        for c in range(n):
            left(tot.at[0, cut(0, n)], dd_s.at[e, c])
    for d in range(1, ntp):
        ring_b(d)
    ring(0, ntp - 1)
    ring(1, 1)
    ring(side, 2)
    for m in range(3):
        local(speed[m], outs_m[m], 9 + m).wait()
        local(weights[m], speed[m], 12 + m).start()

    inverse, scale = scales()

    def eye(shape, shift):
        down = lax.broadcasted_iota(jnp.int32, shape, 0)
        over = lax.broadcasted_iota(jnp.int32, shape, 1)
        return jnp.where(down == over + shift, COEF_ONE, 0.0)

    def product(index, span, lhs, rhs, out, finish, before, after=None):
        step = span // count

        def where(k, who):
            i, j = k // 4, jnp.where(k == 1, 3, jnp.where(k > 1, k - 1 - k // 4 * 2, 0))
            odd = jnp.where(k == 1, 1, 0)
            i, j = i + who * (3 - j + odd - i), j + who * (3 - i - odd - j)
            return i, j, at(i * step, step, step), at(j * step, step, step)

        def compute(k):
            i, j, rows, cols = where(k, r)
            acc = jnp.dot(lhs[rows, :span], rhs[:span, cols], preferred_element_type=F32)
            value = finish(acc, lhs, rows, cols, (j - i) * step).astype(BF16)
            out[rows, cols] = value

            @pl.when(i != j)
            def _():
                out[cols, rows] = value.T

        def ship(k):
            _, _, rows, cols = where(k, r)
            here = out.at[rows, cols]
            send(here, here, pr_s.at[index, k], pr_r.at[index, k], mate).start()

        def take(k):
            i, j, rows, cols = where(k, other)
            here = out.at[rows, cols]
            arrived(here, pr_r.at[index, k])

            @pl.when(i != j)
            def _():
                out[cols, rows] = out[rows, cols].T

            left(here, pr_s.at[index, k])

        compute(0)
        before()
        ship(0)

        def run(k, carry):
            compute(k)
            ship(k)
            return carry

        lax.fori_loop(1, 5, run, 0)
        if after is not None:
            after()
        take(1)

        def rest(n, carry):
            take(n + jnp.minimum(n, 1))
            return carry

        return lambda: lax.fori_loop(0, 4, rest, 0)

    def poly_one(inv):
        def finish(acc, lhs, rows, cols, shift):
            gram_part = lhs[rows, cols].astype(F32) * inv
            return eye(acc.shape, shift) + COEF_THREE * gram_part + COEF_FIVE * (acc * inv * inv)

        return finish

    def times(inv):
        return lambda acc, lhs, rows, cols, shift: acc * inv

    def plain(acc, lhs, rows, cols, shift):
        return acc

    def poly_two(acc, lhs, rows, cols, shift):
        return eye(acc.shape, shift) + COEF_THREE * lhs[rows, cols].astype(F32) + COEF_FIVE * acc

    done = product(0, size, b0, b0, b1, poly_one(inverse), lambda: None)

    blocks = 3

    def block(b, who):
        i, j = (2 * who + b, who) if b < 2 else (who, 1)
        return i * half, j * width

    def branch_gram():
        for d in range(1, ntp):
            arrived(sb.at[:, at(peers[ntp - d] * thin, thin, thin)], ring_r.at[2, d])
        for b in range(blocks):
            def make(who, b=b):
                i, j = block(b, who)
                return lax.dot_general(
                    sb[:, at(i, half, half)],
                    sb[:, at(j, width, width)],
                    (((0,), (0,)), ((), ())),
                    preferred_element_type=F32,
                ).astype(BF16)

            exchange(b, 5 + b, make)

    def settle(b):
        chain_d(b, 5 + b)
        i, j = block(b, r)

        def copy(rows):
            gb[at(i + rows.start, STEP, STEP), at(j, width, width)] = tot[b, rows, :]

        rows_loop(half, STEP, copy)
        here = gb.at[at(i, half, half), at(j, width, width)]
        send(tot.at[b], here, gd_s.at[b], gd_r.at[b], mate).start()

    done = product(1, size, b0, b1, b2, times(inverse), done, branch_gram)

    def begin_chain(first):
        first()
        for b in range(blocks):
            chain_a(b, 5 + b)

    done = product(2, size, b2, b1, b0, plain, functools.partial(begin_chain, done))
    chain_b(0, 5)
    done = product(3, size, b0, b0, b2, poly_two, done)
    chain_b(1, 6)
    chain_c(0, 5)
    done()

    def panel(lhs, rhs, out, span, finish):
        def step(j, carry):
            cols = at(j * tile, tile, tile)
            acc = jnp.dot(lhs(), rhs(cols), preferred_element_type=F32)
            out(cols, finish(acc, cols).astype(BF16))
            return carry

        lax.fori_loop(0, span // tile, step, 0)

    def same(acc, cols):
        return acc

    def factor(rows, begin, extra, g2, p1, p2, span, scaling, out, tasks):
        def buf(ref):
            return lambda: ref[:rows, :span]

        def put(ref):
            def write(cols, value):
                ref[:rows, cols] = value

            return write

        def cubic(acc, cols):
            down = lax.broadcasted_iota(jnp.int32, acc.shape, 0)
            over = lax.broadcasted_iota(jnp.int32, acc.shape, 1)
            down = down + jnp.where(down < half, begin, extra - half)
            unit = jnp.where(down == over + cols.start, COEF_ONE, 0.0)
            return unit + COEF_THREE * c1[:rows, cols].astype(F32) + COEF_FIVE * acc

        panel(buf(c2), p2, put(c0), span, same)
        tasks(0)
        panel(buf(c0), g2, put(c1), span, same)
        tasks(1)
        panel(buf(c1), g2, put(c2), span, same)
        tasks(2)
        panel(buf(c2), p2, put(c0), span, same)
        tasks(3)
        panel(buf(c0), p2, put(c2), span, cubic)
        tasks(4)
        panel(buf(c2), p2, put(c0), span, same)
        tasks(5)
        panel(buf(c0), p1, out, span, lambda acc, cols: acc * scaling)

    def view(ref, top, span):
        return lambda cols: ref[top : top + span, cols]

    slab = half // nfs
    begin, extra = t * width + r * half, across * width + r * half + f * slab

    chunk = size // 2

    def strip(m, who, j, c):
        return qt.at[m, at(who * half + j * slab, slab, slab), c * chunk : (c + 1) * chunk]

    def depart(c):
        piece = qs.at[:, c * chunk : (c + 1) * chunk]
        send(piece, strip(side, r, f, c), x_s.at[c], x_r.at[c], {"tp": across}).start()

    def put_q(cols, value):
        qt[side, at(r * half, half, half), cols] = value[:half]
        qs[:, cols] = value[half:]
        pl.when(cols.start == chunk)(lambda: depart(0))

    def put_qb(cols, value):
        qtb[:, cols] = value

    def fill(rows):
        c2[rows, :] = b2[at(begin + rows.start, STEP, STEP), :]

    rows_loop(half, STEP, fill)
    c2[half : half + slab, :] = b2[at(extra, slab, slab), :]

    def tasks(n):
        if n == 0:
            chain_b(2, 7)
        if n == 1:
            chain_c(1, 6)
        if n == 2:
            chain_c(2, 7)
        if n == 3:
            settle(0)
        if n == 5:
            settle(1)
            settle(2)

    factor(
        half + slab, begin, extra, view(b0, 0, size), view(b1, 0, size), view(b2, 0, size),
        size, scale, put_q, tasks,
    )

    depart(1)
    landing = qt.at[side, at(r * half, half, half)]
    send(landing, landing, q_s, q_r, mate).start()

    def course(d, up):
        j, ahead = (f - d, f + 1) if up else (f + d, f - 1)
        inside = jnp.logical_and(j >= 0, j < nfs)
        more = jnp.logical_and(ahead >= 0, ahead < nfs)
        return 0 if up else 1, j, ahead, inside, more

    def pass_on(d, c, up):
        lane, j, ahead, inside, more = course(d, up)

        def onward(spot):
            send(
                spot, spot, st_s.at[lane, 2 * d + c], st_r.at[lane, 2 * d + 2 + c], {"fs": ahead}
            ).start()

        if d == 0:
            pl.when(more)(lambda: onward(strip(1 - side, r, f, c)))
            return

        @pl.when(inside)
        def _():
            spot = strip(1 - side, r, j, c)
            arrived(spot, st_r.at[lane, 2 * d + c])
            pl.when(more)(lambda: onward(spot))
            send(
                spot, spot, sd_s.at[lane, 2 * d + c], sd_r.at[lane, 2 * d + c], mate
            ).start()

    def travel(d, c):
        if d >= nfs:
            return
        if d == 0:
            arrived(strip(1 - side, r, f, c), x_r.at[c])
        pass_on(d, c, True)
        pass_on(d, c, False)
        if d == 0:
            here = strip(1 - side, r, f, c)
            send(here, here, sd_s.at[0, c], sd_r.at[0, c], mate).start()

    def travelled(d, c, up):
        lane, j, ahead, inside, more = course(d, up)

        @pl.when(inside)
        def _():
            spot = strip(1 - side, other, j, c)
            arrived(spot, sd_r.at[lane, 2 * d + c])
            left(spot, sd_s.at[lane, 2 * d + c])

    def sent_on(d, c, up):
        lane, j, ahead, inside, more = course(d, up)
        pl.when(jnp.logical_and(inside, more))(
            lambda: left(strip(1 - side, r, j, c), st_s.at[lane, 2 * d + c])
        )

    for b in range(blocks):
        i, j = block(b, other)
        arrived(gb.at[at(i, half, half), at(j, width, width)], gd_r.at[b])
    sums[...] = jnp.zeros_like(sums)
    survey(gb, 0, 0, True, width)
    survey(gb, width, width, True, width)
    survey(gb, 0, width, False, width)
    gb[width:, :width] = gb[:width, width:].T
    inverse_b, scale_b = scales()
    def square(lhs, rhs, out, finish):
        def step(n, carry):
            i, j = n // 2, (n + 1) // 2
            rows, cols = at(i * width, width, width), at(j * width, width, width)
            acc = jnp.dot(lhs[rows, :small], rhs[:small, cols], preferred_element_type=F32)
            value = finish(acc, lhs, rows, cols, (j - i) * width).astype(BF16)
            out[rows, cols] = value

            @pl.when(i != j)
            def _():
                out[cols, rows] = value.T

            return carry

        lax.fori_loop(0, 3, step, 0)

    square(gb, gb, b1, poly_one(inverse_b))
    square(gb, b1, b2, times(inverse_b))
    travel(0, 0)
    square(b2, b1, b0, plain)
    travel(0, 1)
    square(b0, b0, b2, poly_two)
    travel(1, 0)
    c2[:thin, :small] = b2[at(t * thin, thin, thin), :small]

    def tasks_b(n):
        if n == 1:
            travel(1, 1)
        if n == 3:
            travel(2, 0)
        if n == 5:
            travel(2, 1)

    factor(
        thin, t * thin, 0, view(b0, 0, small), view(b1, 0, small), view(b2, 0, small),
        small, scale_b, put_qb, tasks_b,
    )

    def update(m, lhs, rhs, rate, ref, rows_of, step):
        def body(rows):
            acc = lax.dot_general(
                lhs(rows), rhs(), (((1,), (1,)), ((), ())), preferred_element_type=F32
            )
            ref(rows, acc, rate)

        rows_loop(rows_of, step, body)

    def put_big(m):
        def write(rows, acc, rate):
            vel[m, rows, :] = SHRINK * vel[m, rows, :] - rate * acc

        return write

    def put_small(rows, acc, rate):
        velb[rows, :] = SHRINK * velb[rows, :] - rate * acc

    rate = RATE * math.sqrt(height * nfs * 2)
    rate_b = RATE * math.sqrt(low * nfs * 2)

    def finish_big(m):
        update(m, lambda rows: s[m, rows, :], lambda: qt[m], rate, put_big(m), height, CHUNK)

        @pl.when(m == 0)
        def _():
            local(speed[0], gu, 15).start()

        @pl.when(m == 1)
        def _():
            local(speed[1], uu, 16).start()

    for m in range(3):
        local(weights[m], speed[m], 12 + m).wait()
    update(2, lambda rows: sb[rows, :], lambda: qtb[...], rate_b, put_small, low, CHUNK)
    local(velb, bu, 17).start()
    ring_in(0, ntp - 1)
    ring_in(1, 1)
    ring_in(1 - side, 2)
    arrived(qt.at[side, at(other * half, half, half)], q_r)
    finish_big(side)
    for d in range(3, nfs):
        travel(d, 0)
        travel(d, 1)
    for d in range(nfs):
        for c in range(2):
            travelled(d, c, True)
            if d > 0:
                travelled(d, c, False)
    finish_big(1 - side)

    for m in range(3):
        for d in range(1, ntp):
            block = s.at[m, :, mine] if m < 2 else sb.at[:, mine_b]
            left(block, ring_s.at[m, d])
    for b in range(blocks):
        chain_end(b, 5 + b)
        left(tot.at[b], gd_s.at[b])
    left(landing, q_s)
    for c in range(2):
        left(qs.at[:, c * chunk : (c + 1) * chunk], x_s.at[c])
        for d in range(nfs - 1):
            sent_on(d, c, True)
            sent_on(d, c, False)
    local(speed[0], gu, 15).wait()
    local(speed[1], uu, 16).wait()
    local(velb, bu, 17).wait()


def hand_over(*refs):
    count = (len(refs) - 2) // 3
    sources, targets, stages = refs[:count], refs[count : 2 * count], refs[2 * count : 3 * count]
    came, went = refs[3 * count :]
    moves = []
    for i in range(count):
        rows = sources[i].shape[0]
        for j, top in enumerate((0, rows // 2)):
            span = pl.ds(top, rows // 2)
            stage = stages[i].at[span]
            moves.append(
                (
                    pltpu.make_async_copy(sources[i].at[span], stage, came.at[i, j]),
                    pltpu.make_async_copy(stage, targets[i].at[span], went.at[i, j]),
                )
            )
    for take, _ in moves:
        take.start()
    for take, give in moves:
        take.wait()
        give.start()
    for _, give in moves:
        give.wait()


def local_part(nfs, ntp, *args):
    height, width = args[1].shape
    low, thin = args[7].shape
    size, small = width * ntp, thin * ntp
    half = width // 2
    blocks = 3
    vmem = pltpu.VMEM
    dma = pltpu.SemaphoreType.DMA
    scratch = [
        vmem((2, height, size), BF16),
        vmem((low, small), BF16),
        vmem((2, height, width), F32),
        vmem((low, thin), F32),
        vmem((2, height, width), F32),
        vmem((low, thin), F32),
        vmem((2, height, width), F32),
        vmem((low, thin), F32),
    ]
    scratch += [vmem((5, half, width), BF16)] * 4
    scratch += [vmem((5 + blocks, half, width), BF16), vmem((5, half, width), BF16)]
    scratch += [vmem((size, size), BF16)] * 3 + [vmem((small, small), BF16)]
    scratch += [vmem((half + half // nfs, size), BF16)] * 3 + [vmem((half // nfs, size), BF16)]
    scratch += [vmem((2, width, size), BF16), vmem((thin, small), BF16), vmem((2, 8, width), F32)]
    slots = dma((5 + blocks,))
    scratch += [dma((18,)), dma((3,)), dma((3,)), dma((3, ntp)), dma((3, ntp))]
    scratch += [slots] * 2 + [dma((5 + blocks, 4))] * 5
    scratch += [dma((5, 4, 2)), dma((10, 4)), dma((10, 4)), dma((10, 4)), dma((blocks,)), dma((blocks,))]
    scratch += [dma((4, 5))] * 2 + [dma, dma, dma((2,)), dma((2,))] + [dma((2, 2 * nfs))] * 4
    outs = []
    for i in range(3):
        outs += [jax.ShapeDtypeStruct(args[3 * i + 1].shape, F32)] * 2
    results = pl.pallas_call(
        functools.partial(kernel, nfs, ntp),
        out_shape=tuple(outs),
        in_specs=[pl.BlockSpec(memory_space=pl.ANY)] * 9,
        out_specs=tuple([pl.BlockSpec(memory_space=pl.ANY)] * 6),
        scratch_shapes=scratch,
        compiler_params=pltpu.CompilerParams(
            collective_id=0, has_side_effects=True, vmem_limit_bytes=GRANT
        ),
        name="orthogonal",
    )(*args)
    dma2 = dma((len(outs), 2))
    return pl.pallas_call(
        hand_over,
        out_shape=tuple(outs),
        in_specs=[pl.BlockSpec(memory_space=pl.ANY)] * len(outs),
        out_specs=tuple([pl.BlockSpec(memory_space=pl.ANY)] * len(outs)),
        scratch_shapes=[vmem(o.shape, F32) for o in outs] + [dma2, dma2],
        name="hand_over",
    )(*results)


def solution(mesh):
    sizes = mesh.shape
    split = P(("fs", "rep"), "tp")
    return jax.shard_map(
        functools.partial(local_part, sizes["fs"], sizes["tp"]),
        mesh=mesh,
        in_specs=(P("rep", "fs", "tp"), split, split) * 3,
        out_specs=(split,) * 6,
        check_vma=False,
    )
```
